128 devices in a mesh: sp: 16 (over z, x), tp: 8 (over y, core).
Axes of the slice: x: 4, y: 4, z: 4, core: 2. Of those that a mesh axis runs over, the one named last changes fastest.
Arguments:
- block_input: bfloat16 [32768, 4096], P('sp'), may hold values from -6 to 6
- value_weight: bfloat16 [4096, 1024], P(None, 'tp'), may hold values from -0.09375 to 0.09375
- key_rows: bfloat16 [32768, 512], P('sp', 'tp'), may hold values from -1 to 1
- query_rows: bfloat16 [32768, 512], P('sp', 'tp'), may hold values from -1 to 1
- decay_pre: float32 [16, 32768], P('tp', 'sp'), may hold values from -3 to 2
- decay_log: float32 [16], P('tp'), may hold values from -16 to -2
- gate_rows: bfloat16 [32768, 1024], P('sp', 'tp'), may hold values from -6 to 6
- out_grad: bfloat16 [32768, 1024], P('sp', 'tp'), may hold values from -6 to 6
Outputs:
- key_grad: float32 [32768, 512], P('sp', 'tp')
- query_grad: float32 [32768, 512], P('sp', 'tp')
- decay_grad: float32 [16, 32768], P('tp', 'sp')
- gate_grad: float32 [32768, 1024], P('sp', 'tp')
- weight_grad: float32 [4096, 1024], P('sp', 'tp')
- row_norms: float32 [4096], P('sp')
The draws below stay inside these ranges and needn't reach their ends.
All inputs are finite; a program needn't handle non-finite values.
Results may differ from the reference program's by a relative error of at most 0.0035.
Values sent between devices are 32-bit elements; how exact they have to be, the bound alone decides.
No kernel may reach another device: no remote copies, remote signals or barrier semaphores. Data moves between devices by JAX's collectives and lax.ppermute only.
A program may use at most 128 MiB of HBM per device.

```python
import jax
import jax.numpy as jnp
from jax import lax

D = 4096
HEADS = 16
HEAD = 64
GROUPS = 8
STATE = 64
BLK = 128
TOK_DEV = 2048
TOKENS = 32768


def draw_decay_log(key, part):
    pick_key, slow_key, fast_key = jax.random.split(jax.random.fold_in(key, 11), 3)
    slow_share = 0.5
    is_slow = jax.random.uniform(pick_key, (HEADS,), jnp.float32) < slow_share
    slow_rate = jax.random.uniform(slow_key, (HEADS,), jnp.float32, 0.25, 0.5) / TOKENS
    fast_rate = jax.random.uniform(fast_key, (HEADS,), jnp.float32, 0.05, 0.1)
    return jnp.log(jnp.where(is_slow, slow_rate, fast_rate)).astype(jnp.float32)


def draw_decay_pre(key, part):
    level_key, noise_key = jax.random.split(jax.random.fold_in(key, 23), 2)
    levels = jax.random.uniform(level_key, (HEADS, TOKENS // TOK_DEV), jnp.float32, -1.5, 1.0)
    noise = jax.random.uniform(noise_key, (HEADS, TOKENS), jnp.float32, -0.99, 0.99)
    return (jnp.repeat(levels, TOK_DEV, axis=1) + noise).astype(jnp.float32)


def raised(array, key, source, target, blocks, factor):
    def block_of(position):
        return (jnp.arange(array.shape[position]) // (array.shape[position] // blocks)).reshape((-1,) + (1,) * (array.ndim - 1 - position))

    one_side = jax.random.permutation(key, blocks)[block_of(target)]
    other_side = (block_of(target) + blocks // 2) % blocks
    return jnp.where((block_of(source) == one_side) | (block_of(source) == other_side), factor * array, array)


def steps_of(stream_key, shape, cuts, least, high):
    factor_of, own = 1.0, jax.random.fold_in(stream_key, 6)
    for dim, shards_of in cuts:
        heights = jnp.exp(jax.random.uniform(jax.random.fold_in(own, dim), (shards_of,), jnp.float32, least / len(cuts), high / len(cuts)))
        factor_of = factor_of * jnp.repeat(heights, shape[dim] // shards_of).reshape([-1 if axis == dim else 1 for axis in range(len(shape))])
    return factor_of


def bell_draw(key, shape, width, most, cuts=(), dtype=jnp.bfloat16):
    level = steps_of(key, shape, cuts, -0.22, 0.18) if cuts else 1.0
    drawn = jax.random.normal(key, shape, jnp.float32) * width * level
    return jnp.minimum(jnp.maximum(drawn, -most), most).astype(dtype)


def noise_with(own_key, dims, scale, most, cuts, heavy, kind=jnp.bfloat16):
    entries = scale * jax.random.normal(own_key, dims, jnp.float32)
    if cuts:
        entries = entries * steps_of(own_key, dims, cuts, -0.22, 0.18)
    return jnp.clip(raised(entries, jax.random.fold_in(own_key, 3), *heavy), -most, most).astype(kind)


def setup_inputs(seed: int = 0) -> dict:
    arg_keys = jax.random.split(jax.random.key(seed), 9)
    return {
        "block_input": noise_with(arg_keys[0], (TOKENS, D), 1.0, 6.0, ((0, 16),), (0, 1, 16, 2.0)),
        "value_weight": bell_draw(arg_keys[1], (D, HEADS * HEAD), D ** -0.5, 0.09375, ((1, 8),)),
        "key_rows": bell_draw(arg_keys[2], (TOKENS, GROUPS * STATE), 0.125, 1.0, ((0, 16), (1, 8))),
        "query_rows": bell_draw(arg_keys[3], (TOKENS, GROUPS * STATE), 0.125, 1.0, ((0, 16), (1, 8))),
        "decay_pre": draw_decay_pre(jax.random.fold_in(arg_keys[8], 71), 0),
        "decay_log": draw_decay_log(jax.random.fold_in(arg_keys[8], 71), 0),
        "gate_rows": bell_draw(arg_keys[6], (TOKENS, HEADS * HEAD), 1.0, 6.0, ((0, 16), (1, 8))),
        "out_grad": bell_draw(arg_keys[7], (TOKENS, HEADS * HEAD), 1.0, 6.0, ((0, 16), (1, 8))),
    }


HIGH = lax.Precision.HIGHEST

def block_mixer(values, key_float, query_float, step_sizes, log_steps, start_state):
    length, head_count, head_width = values.shape
    groups = key_float.shape[1]
    group_ratio = head_count // groups
    blocks = length // BLK
    value_blocks = values.reshape(blocks, BLK, head_count, head_width)
    key_blocks = jnp.repeat(key_float.reshape(blocks, BLK, groups, -1), group_ratio, axis=2)
    query_blocks = jnp.repeat(query_float.reshape(blocks, BLK, groups, -1), group_ratio, axis=2)
    step_blocks = step_sizes.reshape(head_count, blocks, BLK).transpose(1, 0, 2)
    running = jnp.cumsum(log_steps.reshape(head_count, blocks, BLK).transpose(1, 0, 2), axis=-1)
    lower = jnp.tril(jnp.ones((BLK, BLK), bool))
    spread = jnp.where(lower, running[..., :, None] - running[..., None, :], 0.0)
    decay = jnp.where(lower, jnp.exp(spread), 0.0)
    scores = jnp.einsum('cqhn,ckhn->chqk', query_blocks, key_blocks, precision=HIGH)
    weights = scores * decay * step_blocks[:, :, None, :]
    inner = jnp.einsum('chqk,ckhp->cqhp', weights, value_blocks, precision=HIGH)
    to_end = jnp.exp(running[..., -1:] - running) * step_blocks
    block_states = jnp.einsum('cqhn,chq,cqhp->chpn', key_blocks, to_end, value_blocks, precision=HIGH)
    factors = jnp.exp(running[..., -1])

    def advance(state_now, item):
        contrib, factor = item
        return (factor[:, None, None] * state_now + contrib, state_now)
    end_state, before = lax.scan(advance, start_state, (block_states, factors))
    outer = jnp.einsum('cqhn,chpn,chq->cqhp', query_blocks, before, jnp.exp(running), precision=HIGH)
    return ((inner + outer).reshape(length, head_count, head_width), end_state)

def reference(block_input, value_weight, key_rows, query_rows, decay_pre, decay_log, gate_rows, out_grad):
    head_count = decay_log.shape[0]
    length = block_input.shape[0]
    groups = key_rows.shape[1] // STATE
    projected = jnp.dot(block_input, value_weight, preferred_element_type=jnp.float32).astype(jnp.bfloat16)
    pre_float = lax.optimization_barrier(projected).astype(jnp.float32)
    sig_pre = jax.nn.sigmoid(pre_float)
    values = (pre_float * sig_pre).reshape(length, head_count, HEAD)
    step_sizes = jax.nn.softplus(decay_pre)
    decay_rates = jnp.exp(decay_log)
    log_steps = -decay_rates[:, None] * step_sizes
    key_float = key_rows.astype(jnp.float32).reshape(length, groups, STATE)
    query_float = query_rows.astype(jnp.float32).reshape(length, groups, STATE)
    gate_float = gate_rows.astype(jnp.float32)
    sig_gate = jax.nn.sigmoid(gate_float)
    cot_float = out_grad.astype(jnp.float32)
    zero_state = jnp.zeros((head_count, HEAD, STATE), jnp.float32)

    def forward(vals, krows, qrows, sizes, logs):
        mixed, _ = block_mixer(vals, krows, qrows, sizes, logs, zero_state)
        return mixed
    mixed, pullback = jax.vjp(forward, values, key_float, query_float, step_sizes, log_steps)
    grad_mixed = (cot_float * gate_float * sig_gate).reshape(length, head_count, HEAD)
    value_back, key_back, query_back, size_back, log_back = pullback(grad_mixed)
    gate_grad = cot_float * mixed.reshape(length, head_count * HEAD) * sig_gate * (1.0 + gate_float * (1.0 - sig_gate))
    size_total = size_back - decay_rates[:, None] * log_back
    decay_grad = size_total * jax.nn.sigmoid(decay_pre)
    value_grad = (value_back.reshape(length, head_count * HEAD) * sig_pre * (1.0 + pre_float * (1.0 - sig_pre))).astype(jnp.bfloat16)
    weight_grad = lax.dot_general(block_input, value_grad, (((0,), (0,)), ((), ())), preferred_element_type=jnp.float32)
    row_norms = lax.optimization_barrier(jnp.sum(weight_grad * weight_grad, axis=1))
    return (key_back.reshape(length, groups * STATE), query_back.reshape(length, groups * STATE), decay_grad, gate_grad, weight_grad, row_norms)
```

```python
import jax
import jax.numpy as jnp
from jax import lax
from jax.experimental import pallas as pl
from jax.experimental.pallas import tpu as pltpu
from jax.sharding import PartitionSpec as P

D = 4096
T = 2048
C = 128
NC = T // C
HEAD = 64
STATE = 64
SP = 16
PAY = 72
F32 = jnp.float32
BF16 = jnp.bfloat16


def dot(a, b, ca=1, cb=0):
    return lax.dot_general(a, b, (((ca,), (cb,)), ((), ())), preferred_element_type=F32)


def split2(x):
    hi = x.astype(BF16)
    return hi, (x - hi.astype(F32)).astype(BF16)


def split3(x):
    hi = x.astype(BF16)
    rest = x - hi.astype(F32)
    mid = rest.astype(BF16)
    return hi, mid, (rest - mid.astype(F32)).astype(BF16)


def iota(shape, dim):
    return lax.broadcasted_iota(jnp.int32, shape, dim)


def exact_dot_r(x, ones):
    hi, mid, lo = split3(x)
    return dot(hi, ones) + dot(mid, ones) + dot(lo, ones)


def sigmoid(x):
    return 1.0 / (1.0 + jnp.exp(-x))


def softplus(x):
    return jnp.maximum(x, 0.0) + jnp.log(1.0 + jnp.exp(-jnp.abs(x)))


def selector():
    row = iota((16, 384), 0)
    lane = iota((16, 384), 1)
    head = row & 1
    block = lane >> 7
    in_r = (row < 6) & (block < 2) & (head == block)
    in_s = (row >= 6) & (row < 12) & (block == 2) & (head == ((lane >> 6) & 1))
    return jnp.where(in_r | in_s, 1.0, 0.0).astype(BF16)


def first_head(shape):
    return iota(shape, 1) < HEAD


def columns(pk, sel):
    cols = dot(pk, sel, 0, 0)
    return cols[:, :128], cols[:, 128:256], cols[:, 256:]


def by_head(row0, row1, width=128):
    return jnp.where(first_head((row0.shape[0], width)), row0, row1)


def zero_other(x, keep_first):
    m = first_head(x.shape)
    z = jnp.zeros_like(x)
    return jnp.where(m, x, z) if keep_first else jnp.where(m, z, x)


def prepare_kernel(rate_ref, dp_ref, q_ref, gate_ref, og_ref, rows_ref, pk_ref, gh_ref, gl_ref, ds_ref, pay_ref, x_scr):
    for c in range(NC):
        x_scr[2 * c : 2 * c + 2, :] = dp_ref[:, c * C : (c + 1) * C]
    step = softplus(x_scr[...])
    rate = jnp.where((iota((2 * NC, C), 0) & 1) == 0, rate_ref[0], rate_ref[1])
    logs = -rate * step
    upto = jnp.where(iota((C, C), 0) <= iota((C, C), 1), 1.0, 0.0).astype(BF16)
    run = exact_dot_r(logs, upto)
    ends = jnp.broadcast_to(run[:, C - 1 : C], (2 * NC, C))
    i, j = iota((2 * NC, 2 * NC), 0), iota((2 * NC, 2 * NC), 1)
    same = (i & 1) == (j & 1)
    below = jnp.where(same & (j < i), 1.0, 0.0).astype(BF16)
    above = jnp.where(same & (j > i), 1.0, 0.0).astype(BF16)
    e3 = split3(ends)
    before = dot(below, e3[0]) + dot(below, e3[1]) + dot(below, e3[2])
    after = dot(above, e3[0]) + dot(above, e3[1]) + dot(above, e3[2])
    r3, s3 = split3(run), split3(step)
    for c in range(NC):
        p = slice(2 * c, 2 * c + 2)
        rows_ref[c] = jnp.concatenate([run[p], step[p], before[p], after[p]], axis=0)
        pk_ref[c] = jnp.concatenate(
            [a[p].astype(F32) for a in (*r3, *s3)] + [jnp.zeros((4, C), F32)], axis=0
        ).astype(BF16)
    sel = selector()

    def chunk(n, state):
        c = NC - 1 - n
        at = pl.ds(pl.multiple_of(c * C, C), C)
        gate = gate_ref[at, :].astype(F32)
        g = og_ref[at, :].astype(F32) * gate * sigmoid(gate)
        gh, gl = split2(g)
        gh_ref[at, :] = gh
        gl_ref[at, :] = gl
        r0, r1, _ = columns(pk_ref[c], sel)
        gs = g * jnp.exp(by_head(r0, r1))
        hi, lo = split2(gs)
        q = q_ref[at, :]
        part = dot(q, hi, 0, 0) + dot(q, lo, 0, 0)
        ds_ref[c] = state
        rows = rows_ref[c]
        end = by_head(rows[0:1, C - 1 : C], rows[1:2, C - 1 : C])
        return part + jnp.exp(end) * state

    total = lax.fori_loop(0, NC, chunk, jnp.zeros((STATE, 128), F32), unroll=4)
    logsum = by_head(before[2 * NC - 2 : 2 * NC - 1] + ends[2 * NC - 2 : 2 * NC - 1], before[2 * NC - 1 :] + ends[2 * NC - 1 :])
    piece = jnp.concatenate([total, jnp.broadcast_to(logsum, (PAY - STATE, 128))], axis=0)
    for n in range(SP):
        pay_ref[n] = piece


TT = 256
PER = TT // C


def inner_kernel(x_ref, w_ref, q_ref, k_ref, gh_ref, gl_ref, rows_ref, pk_ref,
                 pre_ref, y_ref, p1_ref, p2_ref, dq_ref, dk_ref, out_rows_ref, s_ref, pay_ref, s_scr):
    n = pl.program_id(0)

    @pl.when(n == 0)
    def _():
        s_scr[...] = jnp.zeros_like(s_scr)

    projected = dot(x_ref[...], w_ref[...]).astype(BF16)
    pre_ref[...] = projected
    sel = selector()
    t, s = iota((C, C), 0), iota((C, C), 1)
    lower = t >= s
    strict = jnp.where(t < s, 1.0, 0.0).astype(BF16)
    for m in range(PER):
        at = slice(m * C, (m + 1) * C)
        pre = projected[at].astype(F32)
        sig = sigmoid(pre)
        v = pre * sig
        slope = sig * (1.0 + pre * (1.0 - sig))
        vh, vl = split2(v)
        q, k = q_ref[at, :], k_ref[at, :]
        gh, gl = gh_ref[at, :], gl_ref[at, :]
        rows = rows_ref[m]
        rc0, rc1, stp = columns(pk_ref[m], sel)
        scores = dot(q, k, 1, 1)
        d0 = jnp.where(lower, jnp.exp(rc0 - rows[0:1]), 0.0) * rows[2:3]
        d1 = jnp.where(lower, jnp.exp(rc1 - rows[1:2]), 0.0) * rows[3:4]
        w0, w1 = scores * d0, scores * d1
        w0b, w1b = w0.astype(BF16), w1.astype(BF16)
        wide = jnp.concatenate([w0b, w1b], axis=1)
        tall = jnp.concatenate([w0b, w1b], axis=0)
        vh2 = jnp.concatenate([zero_other(vh, True), zero_other(vh, False)], axis=0)
        vl2 = jnp.concatenate([zero_other(vl, True), zero_other(vl, False)], axis=0)
        gh2 = jnp.concatenate([zero_other(gh, True), zero_other(gh, False)], axis=0)
        gl2 = jnp.concatenate([zero_other(gl, True), zero_other(gl, False)], axis=0)
        y_ref[at, :] = dot(wide, vh2) + dot(wide, vl2)
        dv = dot(tall, gh2, 0, 0) + dot(tall, gl2, 0, 0)
        gv = dot(jnp.concatenate([gh2, gl2], axis=1), jnp.concatenate([vh, vh], axis=1), 1, 1)
        gv0, gv1 = gv[:C], gv[C:]
        dh, dl = split2(gv0 * d0 + gv1 * d1)
        dq_ref[at, :] = dot(jnp.concatenate([dh, dl], axis=1), jnp.concatenate([k, k], axis=0))
        dk_ref[at, :] = dot(jnp.concatenate([dh, dl], axis=0), jnp.concatenate([q, q], axis=0), 0, 0)
        a0, a1 = w0 * gv0, w1 * gv1
        am = dot(jnp.concatenate([a0.astype(BF16), a1.astype(BF16)], axis=0), strict)
        zero = jnp.zeros((C, C), F32)
        out_rows_ref[m] = jnp.concatenate(
            [
                jnp.sum(a0, axis=0, keepdims=True),
                jnp.sum(a1, axis=0, keepdims=True),
                jnp.sum(jnp.where(lower, am[:C], zero), axis=0, keepdims=True),
                jnp.sum(jnp.where(lower, am[C:], zero), axis=0, keepdims=True),
                jnp.zeros((4, C), F32),
            ],
            axis=0,
        )
        end = by_head(rows[0:1, C - 1 : C], rows[1:2, C - 1 : C])
        w = jnp.exp(end - by_head(rc0, rc1)) * stp
        p1_ref[at, :] = dv * slope
        p2_ref[at, :] = w * slope
        hi, lo = split2(v * w)
        part = dot(k, hi, 0, 0) + dot(k, lo, 0, 0)
        state = s_scr[...]
        s_ref[m] = state
        s_scr[...] = jnp.exp(end) * state + part

    @pl.when(n == pl.num_programs(0) - 1)
    def _():
        piece = jnp.concatenate([s_scr[...], jnp.zeros((PAY - STATE, 128), F32)], axis=0)
        for i in range(SP):
            pay_ref[i] = piece


def suffix_state(own, pay_ref, states):
    acc = jnp.zeros((STATE, 128), F32)
    for j in range(SP - 1, 0, -1):
        total = jnp.exp(pay_ref[j, STATE : STATE + 1, :])
        acc = jnp.where(j > own, states(j) + total * acc, acc)
    return acc


def prefix_state(own, pay_ref, states):
    acc = jnp.zeros((STATE, 128), F32)
    for j in range(SP - 1):
        total = jnp.exp(pay_ref[j, STATE : STATE + 1, :])
        acc = jnp.where(j < own, states(j) + total * acc, acc)
    return acc


DT = 512
HALF = 128


def weight_kernel(own_ref, x_ref, k_ref, p1_ref, p2_ref, rows_ref, ds_ref, pay_ref, *refs):
    a_refs, b_refs = refs[0:4], refs[4:8]
    out_state_ref, vg_scr = refs[8], refs[9]
    n = pl.program_id(0)
    own = own_ref[0]

    @pl.when(n == 0)
    def _():
        outgoing = suffix_state(own, pay_ref, lambda j: pay_ref[j, :STATE, :])
        out_state_ref[...] = outgoing
        for c in range(NC):
            at = slice(c * C, (c + 1) * C)
            rows = rows_ref[c]
            state = ds_ref[c] + jnp.exp(by_head(rows[6:7], rows[7:8])) * outgoing
            hi, lo = split2(state)
            k = k_ref[at, :]
            carried = dot(jnp.concatenate([k, k], axis=1), jnp.concatenate([hi, lo], axis=0))
            grad = p1_ref[at, :] + p2_ref[at, :] * carried
            vg_scr[:, at] = grad.T.astype(BF16)

    part = dot(vg_scr[...], x_ref[...])
    z, x = own // 4, own % 4
    for m in range(DT // 256):
        owner = n * (DT // 256) + m
        oz, ox = owner // 4, owner % 4
        dz, dx = (oz - z + 4) % 4, (ox - x + 4) % 4
        first = part[:, m * 256 : m * 256 + HALF]
        second = part[:, m * 256 + HALF : (m + 1) * 256]
        for d in range(4):
            @pl.when(dz == d)
            def _():
                a_refs[d][ox] = first

            @pl.when(dx == d)
            def _():
                b_refs[d][oz] = second


def outer_kernel(own_ref, rate_ref, dp_ref, q_ref, k_ref, gh_ref, gl_ref, gate_ref, og_ref, pre_ref, y_ref,
                 dq_ref, dk_ref, rows_ref, pk_ref, in_rows_ref, s_ref, ds_ref, out_ref, logs_ref, pay_ref,
                 dq_out, dk_out, decay_out, gate_out, in_scr, row_scr, flat_scr):
    n = pl.program_id(0)
    own = own_ref[0]

    @pl.when(n == 0)
    def _():
        in_scr[...] = prefix_state(own, logs_ref, lambda j: pay_ref[j, :STATE, :])

    sel = selector()
    incoming, outgoing = in_scr[...], out_ref[...]
    row, lane = iota((16, 512), 0), iota((16, 512), 1)
    pick = jnp.where((row < 4) & ((row >> 1) == (lane >> 8)) & ((row & 1) == ((lane >> 6) & 1)), 1.0, 0.0).astype(BF16)
    for m in range(PER):
        at = slice(m * C, (m + 1) * C)
        rows = rows_ref[m]
        rc0, rc1, stp = columns(pk_ref[m], sel)
        rc = by_head(rc0, rc1)
        end = by_head(rows[0:1, C - 1 : C], rows[1:2, C - 1 : C])
        grow = jnp.exp(rc)
        w = jnp.exp(end - rc) * stp
        state = s_ref[m] + jnp.exp(by_head(rows[4:5], rows[5:6])) * incoming
        back = ds_ref[m] + jnp.exp(by_head(rows[6:7], rows[7:8])) * outgoing
        sh, sl = split2(state)
        bh, bl = split2(back)
        q, k = q_ref[at, :], k_ref[at, :]
        g = gh_ref[at, :].astype(F32) + gl_ref[at, :].astype(F32)
        pre = pre_ref[at, :].astype(F32)
        v = pre * sigmoid(pre)
        yo = grow * dot(jnp.concatenate([q, q], axis=1), jnp.concatenate([sh, sl], axis=0))
        vo = w * dot(jnp.concatenate([k, k], axis=1), jnp.concatenate([bh, bl], axis=0))
        gate = gate_ref[at, :].astype(F32)
        sg = sigmoid(gate)
        gate_out[at, :] = og_ref[at, :].astype(F32) * (y_ref[at, :] + yo) * sg * (1.0 + gate * (1.0 - sg))
        geh, gel = split2(g * grow)
        dq_out[at, :] = dq_ref[at, :] + dot(jnp.concatenate([geh, gel], axis=1), jnp.concatenate([sh, sh], axis=1), 1, 1)
        vwh, vwl = split2(v * w)
        dk_out[at, :] = dk_ref[at, :] + dot(jnp.concatenate([vwh, vwl], axis=1), jnp.concatenate([bh, bh], axis=1), 1, 1)
        yh, yl = split2(yo * g)
        ch, cl = split2(vo * v)
        picked = dot(pick, jnp.concatenate([yh, yl, ch, cl], axis=1), 1, 1)
        through = jnp.sum(state * back, axis=0, keepdims=True) * jnp.exp(end)
        row_scr[n * PER + m] = jnp.concatenate([picked[:4], through, jnp.zeros((3, C), F32)], axis=0)

    @pl.when(n == pl.num_programs(0) - 1)
    def _():
        t, s = iota((C, C), 0), iota((C, C), 1)
        for c in range(NC):
            p = slice(2 * c, 2 * c + 2)
            r = row_scr[c]
            flat_scr[0, p, :] = r[0:2]
            flat_scr[1, p, :] = r[2:4]
            flat_scr[2, p, :] = jnp.concatenate([zero_other(r[4:5], True), zero_other(r[4:5], False)], axis=0)
            flat_scr[3, p, :] = in_rows_ref[c, 0:2, :]
            flat_scr[4, p, :] = in_rows_ref[c, 2:4, :]
            flat_scr[5, p, :] = dp_ref[:, c * C : (c + 1) * C]
        at_or_after = jnp.where(t >= s, 1.0, 0.0).astype(BF16)
        before = jnp.where(t < s, 1.0, 0.0).astype(BF16)
        every = jnp.ones((C, C), BF16)
        yog, cs = flat_scr[0], flat_scr[1]
        log_back = (
            flat_scr[4] + exact_dot_r(yog, at_or_after) + exact_dot_r(cs, before) + exact_dot_r(flat_scr[2], every)
        )
        dp = flat_scr[5]
        size_back = (flat_scr[3] + cs) / softplus(dp)
        rate = jnp.where((iota((2 * NC, C), 0) & 1) == 0, rate_ref[0], rate_ref[1])
        flat_scr[0] = (size_back - rate * log_back) * sigmoid(dp)
        for c in range(NC):
            decay_out[:, c * C : (c + 1) * C] = flat_scr[0, 2 * c : 2 * c + 2, :]


def finish_kernel(*refs):
    a_refs, b_refs, w_ref, n_ref = refs[0:4], refs[4:8], refs[8], refs[9]
    a = a_refs[0][...] + a_refs[1][...] + a_refs[2][...] + a_refs[3][...]
    b = b_refs[0][...] + b_refs[1][...] + b_refs[2][...] + b_refs[3][...]
    w_ref[:HALF, :] = a.T
    w_ref[HALF:, :] = b.T
    n_ref[0:1, :] = jnp.sum(a * a, axis=0, keepdims=True)
    n_ref[1:2, :] = jnp.sum(b * b, axis=0, keepdims=True)


def sds(shape, dtype=F32):
    return jax.ShapeDtypeStruct(shape, dtype)


def whole(shape):
    return pl.BlockSpec(shape, lambda *a: (0,) * len(shape))


SMEM = pl.BlockSpec(memory_space=pltpu.SMEM)
LIMIT = 56 * 1024 * 1024


def cost(flops, nbytes):
    return pl.CostEstimate(flops=int(flops), transcendentals=0, bytes_accessed=int(nbytes))


def ring(d, along_z):
    if along_z:
        return [(z * 4 + x, ((z + d) % 4) * 4 + x) for z in range(4) for x in range(4)]
    return [(z * 4 + x, z * 4 + (x + d) % 4) for z in range(4) for x in range(4)]


def shards(block_input, value_weight, key_rows, query_rows, decay_pre, decay_log, gate_rows, out_grad):
    own = lax.axis_index("sp").astype(jnp.int32)
    own1 = own.reshape(1)
    rate = jnp.exp(decay_log)
    params = pltpu.CompilerParams(vmem_limit_bytes=LIMIT)

    rows, pk, gh, gl, ds, back_pay = pl.pallas_call(
        prepare_kernel,
        out_shape=(
            sds((NC, 8, C)), sds((NC, 16, C), BF16), sds((T, 128), BF16), sds((T, 128), BF16),
            sds((NC, STATE, 128)), sds((SP, PAY, 128)),
        ),
        in_specs=[SMEM] + [pl.BlockSpec(memory_space=pltpu.VMEM)] * 4,
        scratch_shapes=[pltpu.VMEM((2 * NC, C), F32)],
        compiler_params=params,
        cost_estimate=cost(2e9, 4e6),
        name="prepare",
    )(rate, decay_pre, query_rows, gate_rows, out_grad)

    back_all = lax.all_to_all(back_pay, "sp", 0, 0, tiled=True)

    tok = lambda width: pl.BlockSpec((TT, width), lambda i: (i, 0))
    per = lambda r, w=C: pl.BlockSpec((PER, r, w), lambda i: (i, 0, 0))
    pre, y_in, p1, p2, dq_in, dk_in, in_rows, s_in, fwd_pay = pl.pallas_call(
        inner_kernel,
        grid=(T // TT,),
        out_shape=(
            sds((T, 128), BF16), sds((T, 128)), sds((T, 128)), sds((T, 128)), sds((T, STATE)), sds((T, STATE)),
            sds((NC, 8, C)), sds((NC, STATE, 128)), sds((SP, PAY, 128)),
        ),
        in_specs=[tok(D), whole((D, 128)), tok(STATE), tok(STATE), tok(128), tok(128), per(8), per(16)],
        out_specs=(tok(128), tok(128), tok(128), tok(128), tok(STATE), tok(STATE), per(8), per(STATE, 128), whole((SP, PAY, 128))),
        scratch_shapes=[pltpu.VMEM((STATE, 128), F32)],
        compiler_params=params,
        cost_estimate=cost(9e9, 24e6),
        name="inner",
    )(block_input, value_weight, query_rows, key_rows, gh, gl, rows, pk)

    fixed = lambda shape: whole(shape)
    outs = pl.pallas_call(
        weight_kernel,
        grid=(D // DT,),
        out_shape=tuple(sds((4, 128, HALF)) for _ in range(8)) + (sds((STATE, 128)),),
        in_specs=[
            SMEM, pl.BlockSpec((T, DT), lambda i: (0, i)), fixed((T, STATE)), fixed((T, 128)), fixed((T, 128)),
            fixed((NC, 8, C)), fixed((NC, STATE, 128)), fixed((SP, PAY, 128)),
        ],
        out_specs=tuple(fixed((4, 128, HALF)) for _ in range(8)) + (fixed((STATE, 128)),),
        scratch_shapes=[pltpu.VMEM((128, T), BF16)],
        compiler_params=params,
        cost_estimate=cost(6e9, 24e6),
        name="weight",
    )(own1, block_input, key_rows, p1, p2, rows, ds, back_all)
    a, b, outgoing = outs[0:4], outs[4:8], outs[8]

    z, x = own // 4, own % 4
    a_in = [lax.ppermute(a[d], "sp", ring(d, True)) for d in (1, 3, 2)]
    b_in = [lax.ppermute(b[d], "sp", ring(d, False)) for d in (1, 3, 2)]
    a_sum = a[0] + a_in[0] + a_in[1] + a_in[2]
    b_sum = b[0] + b_in[0] + b_in[1] + b_in[2]
    piece = lambda acc, i: lax.dynamic_index_in_dim(acc, i, 0, keepdims=False)
    a_last = [piece(a_sum, x)] + [lax.ppermute(piece(a_sum, (x + d) % 4), "sp", ring(d, False)) for d in (1, 3, 2)]
    b_last = [piece(b_sum, z)] + [lax.ppermute(piece(b_sum, (z + d) % 4), "sp", ring(d, True)) for d in (1, 3, 2)]

    fwd_all = lax.all_to_all(fwd_pay, "sp", 0, 0, tiled=True)
    key_grad_query = pl.pallas_call(
        outer_kernel,
        grid=(T // TT,),
        out_shape=(sds((T, STATE)), sds((T, STATE)), sds((2, T)), sds((T, 128))),
        in_specs=[
            SMEM, SMEM, fixed((2, T)), tok(STATE), tok(STATE), tok(128), tok(128), tok(128), tok(128), tok(128),
            tok(128), tok(STATE), tok(STATE), per(8), per(16), fixed((NC, 8, C)), per(STATE, 128), per(STATE, 128),
            fixed((STATE, 128)), fixed((SP, PAY, 128)), fixed((SP, PAY, 128)),
        ],
        out_specs=(tok(STATE), tok(STATE), fixed((2, T)), tok(128)),
        scratch_shapes=[pltpu.VMEM((STATE, 128), F32), pltpu.VMEM((NC, 8, C), F32), pltpu.VMEM((6, 2 * NC, C), F32)],
        compiler_params=params,
        cost_estimate=cost(4e9, 10e6),
        name="outer",
    )(own1, rate, decay_pre, query_rows, key_rows, gh, gl, gate_rows, out_grad, pre, y_in, dq_in, dk_in, rows, pk,
      in_rows, s_in, ds, outgoing, back_all, fwd_all)
    query_grad, key_grad, decay_grad, gate_grad = key_grad_query

    weight_grad, norms = pl.pallas_call(
        finish_kernel,
        out_shape=(sds((256, 128)), sds((2, HALF))),
        compiler_params=params,
        cost_estimate=cost(1e6, 1e6),
        name="finish",
    )(*a_last, *b_last)
    norms = norms + lax.ppermute(norms, "tp", [(i, i ^ 1) for i in range(8)])
    others = [lax.ppermute(norms, "tp", [(i, (i + 2 * d) % 8) for i in range(8)]) for d in (1, 3, 2)]
    norms = norms + others[0] + others[1] + others[2]
    return key_grad, query_grad, decay_grad, gate_grad, weight_grad, norms.reshape(256)


def solution(mesh):
    in_specs = (
        P("sp", None), P(None, "tp"), P("sp", "tp"), P("sp", "tp"), P("tp", "sp"), P("tp"), P("sp", "tp"), P("sp", "tp"),
    )
    out_specs = (P("sp", "tp"), P("sp", "tp"), P("tp", "sp"), P("sp", "tp"), P("sp", "tp"), P("sp"))
    return jax.shard_map(shards, mesh=mesh, in_specs=in_specs, out_specs=out_specs, check_vma=False)
```

```python
import jax
import jax.numpy as jnp
from jax import lax
from jax.experimental import pallas as pl
from jax.experimental.pallas import tpu as pltpu
from jax.sharding import PartitionSpec as P

D = 4096
T = 2048
C = 128
NC = T // C
HEAD = 64
STATE = 64
WIDE = 128
SP = 16
PAY = 72
HALF = 128
TT = 256
PER = TT // C
F32 = jnp.float32
BF16 = jnp.bfloat16


def dot(a, b, ca=1, cb=0):
    return lax.dot_general(a, b, (((ca,), (cb,)), ((), ())), preferred_element_type=F32)


def split2(x):
    hi = x.astype(BF16)
    return hi, (x - hi.astype(F32)).astype(BF16)


def split3(x):
    hi = x.astype(BF16)
    rest = x - hi.astype(F32)
    mid = rest.astype(BF16)
    return hi, mid, (rest - mid.astype(F32)).astype(BF16)


def iota(shape, dim):
    return lax.broadcasted_iota(jnp.int32, shape, dim)


def exact_dot_r(x, ones):
    hi, mid, lo = split3(x)
    return dot(hi, ones) + dot(mid, ones) + dot(lo, ones)


def exact_dot_l(ones, x):
    hi, mid, lo = split3(x)
    return dot(ones, hi) + dot(ones, mid) + dot(ones, lo)


def ones_where(mask):
    return jnp.where(mask, 1.0, 0.0).astype(BF16)


def cat(parts, axis):
    return jnp.concatenate(parts, axis=axis)


def sigmoid(x):
    return 1.0 / (1.0 + jnp.exp(-x))


def softplus(x):
    return jnp.maximum(x, 0.0) + jnp.log(1.0 + jnp.exp(-jnp.abs(x)))


def on_lanes(row0, row1):
    return jnp.where(iota((1, WIDE), 1) < HEAD, row0, row1)


def on_rows(row0, row1):
    n = row0.shape[1]
    return jnp.where(iota((WIDE, n), 0) < HEAD, row0, row1)


def head_rows(x):
    return jnp.sum(x[:HEAD], axis=0, keepdims=True), jnp.sum(x[HEAD:], axis=0, keepdims=True)


def rates(decay_log_ref):
    odd = (iota((2 * NC, C), 0) & 1) == 1
    return jnp.exp(jnp.where(odd, decay_log_ref[1], decay_log_ref[0]))


GROW, SHRINK, WHOLE, BEFORE, AFTER = 0, 2, 4, 6, 8


def pair(rows, at):
    return rows[at : at + 1], rows[at + 1 : at + 2]


def halves(shape):
    axis = shape.index(T) if T in shape else shape.index(NC)
    n = shape[axis] // 2
    return [(slice(None),) * axis + (pl.ds(i * n, n),) for i in range(2)]


class Stage:
    def __init__(self, refs, n_scalars, n_raw, n_loads, n_outs, n_first, split):
        counts = (n_scalars, n_raw, n_loads, n_outs, n_loads, n_outs)
        groups, at = [], 0
        for n in counts:
            groups.append(refs[at : at + n])
            at += n
        self.scalars, self.raw, sources, self.targets, self.inputs, self.outs = groups
        self.in_sems, self.out_sems = refs[at], refs[at + 1]
        self.extra = refs[at + 2 :]
        self.waiting = []
        for n, (source, buffer) in enumerate(zip(sources, self.inputs)):
            self.waiting.append([
                pltpu.make_async_copy(source.at[at], buffer.at[at], self.in_sems.at[n, i])
                for i, at in enumerate(halves(buffer.shape) if n in split else [...])
            ])
        for part in range(2):
            self.begin(*range(n_first), part=part)

    def begin(self, *which, part=0):
        for n in which:
            for copy in self.waiting[n][part : part + 1]:
                copy.start()

    def load(self, *which, part=0):
        for n in which:
            for copy in self.waiting[n][part : part + 1]:
                copy.wait()
        got = [self.inputs[n] for n in which]
        return got[0] if len(got) == 1 else got

    def send(self, *which, at=None):
        for n in which:
            source, target = self.outs[n], self.targets[n]
            if at is not None:
                source, target = source.at[at], target.at[at]
            pltpu.make_async_copy(source, target, self.out_sems.at[n]).start()

    def finish(self):
        for n in range(len(self.targets)):
            pltpu.make_async_copy(self.outs[n], self.targets[n], self.out_sems.at[n]).wait()


def front_kernel(st):
    own_ref, decay_log_ref = st.scalars
    x_hbm = st.raw[0]
    flat_scr, x_scr, x_sems = st.extra
    rows_ref, gh_ref, gl_ref, ds_ref, vh_ref, vl_ref, p1_ref, p2_ref, out_rows_ref, s_ref, pay_ref = st.outs
    tiles = T // TT
    copies = []
    for n in range(tiles):
        at = pl.ds(n * TT, TT)
        copies.append(pltpu.make_async_copy(x_hbm.at[at, :], x_scr.at[at, :], x_sems.at[n]))
    st.begin(4, 5)
    for copy in copies:
        copy.start(priority=1)
    dp_ref, q_ref, gate_ref, og_ref = st.load(0, 1, 2, 3)
    for c in range(NC):
        flat_scr[2 * c : 2 * c + 2, :] = dp_ref[:, c * C : (c + 1) * C]
    step = softplus(flat_scr[...])
    logs = -rates(decay_log_ref) * step
    run = exact_dot_r(logs, ones_where(iota((C, C), 0) <= iota((C, C), 1)))
    ends = jnp.broadcast_to(run[:, C - 1 : C], (2 * NC, C))
    i, j = iota((2 * NC, 2 * NC), 0), iota((2 * NC, 2 * NC), 1)
    same = (i & 1) == (j & 1)
    before = exact_dot_l(ones_where(same & (j < i)), ends)
    after = exact_dot_l(ones_where(same & (j > i)), ends)
    tables = (jnp.exp(run), jnp.exp(-run) * step, jnp.exp(ends), jnp.exp(before), jnp.exp(after))
    back = jnp.zeros((STATE, WIDE), F32)
    for c in range(NC - 1, -1, -1):
        rows = cat([a[2 * c : 2 * c + 2] for a in tables], 0)
        rows_ref[c] = cat([rows, jnp.zeros((6, C), F32)], 0)
        at = slice(c * C, (c + 1) * C)
        gate = gate_ref[at, :].astype(F32)
        g = (og_ref[at, :].astype(F32) * gate * sigmoid(gate)).T
        hi, lo = split2(g * on_rows(*pair(rows, GROW)))
        gh_ref[:, at] = hi
        gl_ref[:, at] = lo
        q = q_ref[:, at]
        part = dot(cat([q, q], 1), cat([hi, lo], 1), 1, 1)
        ds_ref[c] = back
        back = part + on_lanes(*pair(rows, WHOLE)) * back
    st.send(0, 1, 2, 3)
    span = jnp.exp(before[2 * NC - 2 :] + ends[2 * NC - 2 :])
    span = jnp.broadcast_to(on_lanes(span[0:1], span[1:2]), (PAY - STATE, WIDE))
    w_ref, k_ref = st.load(4, 5)
    lower = iota((C, C), 0) <= iota((C, C), 1)

    def project(n):
        return dot(x_scr[pl.ds(pl.multiple_of(n * TT, TT), TT), :], w_ref[...]).astype(BF16)

    def chunk(c, projected, state):
        at = pl.ds(pl.multiple_of(c * C, C), C)
        pre = projected.astype(F32).T
        sig = sigmoid(pre)
        v = pre * sig
        slope = sig * (1.0 + pre * (1.0 - sig))
        rows = rows_ref[c]
        shrink = on_rows(*pair(rows, SHRINK))
        vp = v * shrink
        vh, vl = split2(vp)
        vh_ref[:, at] = vh
        vl_ref[:, at] = vl
        q, k = q_ref[:, at], k_ref[:, at]
        scores = jnp.where(lower, dot(k, q, 0, 0), 0.0).astype(BF16)
        dv = dot(cat([gh_ref[:, at], gl_ref[:, at]], 1), cat([scores, scores], 1), 1, 1)
        out_rows_ref[c] = cat([*head_rows(vp * dv), jnp.zeros((6, C), F32)], 0)
        turn = shrink * slope
        p1_ref[:, at] = dv * turn
        p2_ref[:, at] = turn
        s_ref[c] = state
        part = dot(cat([k, k], 1), cat([vh, vl], 1), 1, 1)
        return on_lanes(*pair(rows, WHOLE)) * (state + part)

    def process(n, projected, state):
        for m in range(PER):
            state = chunk(n * PER + m, projected[m * C : (m + 1) * C], state)
        st.send(4, 5, 6, 7, at=(slice(None), pl.ds(pl.multiple_of(n * TT, TT), TT)))
        return state

    def body(n, carry):
        projected, state = carry
        for i in range(1, tiles):
            @pl.when(n == i)
            def _():
                copies[i].wait()
        following = project(n)
        state = process(n - 1, projected, state)
        return following, state

    copies[0].wait()
    first = project(0)
    projected, state = lax.fori_loop(1, tiles, body, (first, jnp.zeros((STATE, WIDE), F32)))
    state = process(tiles - 1, projected, state)
    own = own_ref[0]
    for n in range(SP):
        pay_ref[n] = cat([jnp.where(n > own, state, back), span], 0)
    st.send(8, 9, 10)


def within_kernel(st):
    q_ref, k_ref, gh_ref, gl_ref, vh_ref, vl_ref = st.load(0, 1, 2, 3, 4, 5)
    y_ref, dq_ref, dk_ref, out_rows_ref = st.outs
    lower = iota((C, C), 0) <= iota((C, C), 1)

    def chunk(c, carry):
        at = pl.ds(pl.multiple_of(c * C, C), C)
        q, k = q_ref[:, at], k_ref[:, at]
        gh, gl, vh, vl = gh_ref[:, at], gl_ref[:, at], vh_ref[:, at], vl_ref[:, at]
        scores = jnp.where(lower, dot(k, q, 0, 0), 0.0).astype(BF16)
        y = dot(cat([vh, vl], 1), cat([scores, scores], 0))
        prods = dot(cat([vh, vh], 0), cat([gh, gl], 0), 0, 0) + dot(vl, gh, 0, 0)
        ph, plo = split2(jnp.where(lower, prods, 0.0))
        y_ref[:, at] = y
        dq_ref[:, at] = dot(cat([k, k], 1), cat([ph, plo], 0))
        dk_ref[:, at] = dot(cat([q, q], 1), cat([ph, plo], 1), 1, 1)
        yg = head_rows(y * (gh.astype(F32) + gl.astype(F32)))
        out_rows_ref[c] = cat([*yg, jnp.zeros((6, C), F32)], 0)
        st.send(0, 1, 2, at=(slice(None), at))
        return carry

    lax.fori_loop(0, NC, chunk, 0, unroll=UNROLL)
    st.send(3)


def suffix_state(own, pay_ref):
    acc = jnp.zeros((STATE, WIDE), F32)
    for j in range(SP - 1, 0, -1):
        acc = jnp.where(j > own, pay_ref[j, :STATE, :] + pay_ref[j, STATE : STATE + 1, :] * acc, acc)
    return acc


def prefix_state(own, pay_ref):
    acc = jnp.zeros((STATE, WIDE), F32)
    for j in range(SP - 1):
        acc = jnp.where(j < own, pay_ref[j, :STATE, :] + pay_ref[j, STATE : STATE + 1, :] * acc, acc)
    return acc


ORDER = (1, 3, 2, 0)


def weight_kernel(st):
    own = st.scalars[0][0]
    x_hbm = st.raw[0]
    vg_scr, x_scr, x_sems = st.extra
    z, x = own // 4, own % 4
    tiles = []
    for dz in ORDER:
        for dx in ORDER:
            n = len(tiles)
            oz, ox = (z + dz) % 4, (x + dx) % 4
            at = pl.ds(pl.multiple_of((oz * 4 + ox) * 256, 256), 256)
            copy = pltpu.make_async_copy(x_hbm.at[:, at], x_scr.at[n], x_sems.at[n])
            tiles.append((copy, dz, dx, oz, ox))
    for tile in tiles:
        tile[0].start(priority=1)
    pay_ref, ds_ref, rows_ref, k_ref, p1_ref, p2_ref = st.load(0, 1, 2, 3, 4, 5)
    outgoing = suffix_state(own, pay_ref)
    for c in range(NC):
        at = slice(c * C, (c + 1) * C)
        rows = rows_ref[c]
        back = on_lanes(*pair(rows, WHOLE)) * (ds_ref[c] + on_lanes(*pair(rows, AFTER)) * outgoing)
        k = k_ref[:, at]
        carried = dot(cat(split2(back), 0), cat([k, k], 0), 0, 0)
        vg_scr[:, at] = (p1_ref[:, at] + p2_ref[:, at] * carried).astype(BF16)
    for n, (copy, dz, dx, oz, ox) in enumerate(tiles):
        copy.wait()
        part = dot(vg_scr[...], x_scr[n])
        st.outs[dz][ox] = part[:, :HALF]
        st.outs[4 + dx][oz] = part[:, HALF:]


def outer_kernel(st):
    own_ref, decay_log_ref = st.scalars
    flat_scr = st.extra[0]
    (pay_ref, s_ref, ds_ref, rows_ref, q_ref, k_ref, gh_ref, gl_ref, vh_ref, vl_ref, y_ref, dq_ref, dk_ref,
     gate_ref, og_ref, vdv_ref, yg_ref, dp_ref) = st.load(*range(18))
    dq_out, dk_out, decay_out, gate_out = st.outs
    incoming = prefix_state(own_ref[0], pay_ref)
    outgoing = suffix_state(own_ref[0], pay_ref)

    def chunk(c, carry):
        at = pl.ds(pl.multiple_of(c * C, C), C)
        rows = rows_ref[c]
        state = s_ref[c] + on_lanes(*pair(rows, BEFORE)) * incoming
        back = on_lanes(*pair(rows, WHOLE)) * (ds_ref[c] + on_lanes(*pair(rows, AFTER)) * outgoing)
        sh, sl = split2(state)
        bh, bl = split2(back)
        q, k = q_ref[:, at], k_ref[:, at]
        gh, gl, vh, vl = gh_ref[:, at], gl_ref[:, at], vh_ref[:, at], vl_ref[:, at]
        yo = dot(cat([sh, sl], 0), cat([q, q], 0), 0, 0)
        vo = dot(cat([bh, bl], 0), cat([k, k], 0), 0, 0)
        y = ((y_ref[:, at] + yo) * on_rows(*pair(rows, GROW))).T
        gate = gate_ref[at, :].astype(F32)
        sg = sigmoid(gate)
        gate_out[at, :] = og_ref[at, :].astype(F32) * y * sg * (1.0 + gate * (1.0 - sg))
        dq_out[:, at] = dq_ref[:, at] + dot(cat([sh, sh, sl], 1), cat([gh, gl, gh], 0))
        dk_out[:, at] = dk_ref[:, at] + dot(cat([bh, bh, bl], 1), cat([vh, vl, vh], 0))
        yg = head_rows(yo * (gh.astype(F32) + gl.astype(F32)))
        cs = head_rows(vo * (vh.astype(F32) + vl.astype(F32)))
        through = jnp.sum(state * back, axis=0, keepdims=True)
        first = iota((1, WIDE), 1) < HEAD
        vdv = vdv_ref[c, 0:2, :]
        p = pl.ds(2 * c, 2)
        flat_scr[0, p, :] = cat(yg, 0) + yg_ref[c, 0:2, :] - vdv
        flat_scr[1, p, :] = cat(cs, 0)
        flat_scr[2, p, :] = cat([jnp.where(first, through, 0.0), jnp.where(first, 0.0, through)], 0)
        flat_scr[3, p, :] = vdv
        st.send(0, 1, at=(slice(None), at))
        st.send(3, at=(at, slice(None)))
        return carry

    lax.fori_loop(0, NC // 2, chunk, 0, unroll=UNROLL)
    st.load(*OUTER_SPLIT, part=1)
    lax.fori_loop(NC // 2, NC, chunk, 0, unroll=UNROLL)
    for c in range(NC):
        flat_scr[4, 2 * c : 2 * c + 2, :] = dp_ref[:, c * C : (c + 1) * C]
    t, s = iota((C, C), 0), iota((C, C), 1)
    cs = flat_scr[1]
    log_back = (
        exact_dot_r(flat_scr[0], ones_where(t >= s))
        + exact_dot_r(cs, ones_where(t < s))
        + exact_dot_r(flat_scr[2], jnp.ones((C, C), BF16))
    )
    dp = flat_scr[4]
    size_back = (flat_scr[3] + cs) / softplus(dp)
    flat_scr[0] = (size_back - rates(decay_log_ref) * log_back) * sigmoid(dp)
    for c in range(NC):
        decay_out[:, c * C : (c + 1) * C] = flat_scr[0, 2 * c : 2 * c + 2, :]
    st.send(2)


UNROLL = 4
OUTER_SPLIT = (1, 2, 4, 5, 6, 7, 8, 9, 10, 11, 12, 13, 14)


def finish_kernel(*refs):
    a_refs, b_refs, w_ref, n_ref = refs[0:4], refs[4:8], refs[8], refs[9]
    a = a_refs[0][...] + a_refs[1][...] + a_refs[2][...] + a_refs[3][...]
    b = b_refs[0][...] + b_refs[1][...] + b_refs[2][...] + b_refs[3][...]
    w_ref[:HALF, :] = a.T
    w_ref[HALF:, :] = b.T
    n_ref[0:1, :] = jnp.sum(a * a, axis=0, keepdims=True)
    n_ref[1:2, :] = jnp.sum(b * b, axis=0, keepdims=True)


def sds(shape, dtype=F32):
    return jax.ShapeDtypeStruct(shape, dtype)


SMEM = pl.BlockSpec(memory_space=pltpu.SMEM)
VMEM = pl.BlockSpec(memory_space=pltpu.VMEM)
HBM = pl.BlockSpec(memory_space=pl.ANY)


def staged(kernel, name, scalars, raw, loads, outs, extra=(), flops=1e9, limit=62, first=None, keep=False, split=()):
    first = len(loads) if first is None else first

    def wrapped(*refs):
        if keep:
            at = len(scalars) + len(raw) + len(loads)
            kept, n = refs[at : at + len(outs)], len(loads)
            refs = refs[:at] + refs[at + len(outs) :]
            st = Stage(refs, len(scalars), len(raw), n, 0, first, split)
            st.outs = kept
        else:
            st = Stage(refs, len(scalars), len(raw), len(loads), len(outs), first, split)
        kernel(st)
        st.finish()

    DMA = pltpu.SemaphoreType.DMA
    return pl.pallas_call(
        wrapped, out_shape=tuple(outs), out_specs=tuple([VMEM if keep else HBM] * len(outs)),
        in_specs=[SMEM] * len(scalars) + [HBM] * (len(raw) + len(loads)), name=name,
        scratch_shapes=[pltpu.VMEM(a.shape, a.dtype) for a in (*loads, *(() if keep else outs))]
        + [DMA((max(len(loads), 1), 2)), DMA((len(outs),)), *extra],
        compiler_params=pltpu.CompilerParams(vmem_limit_bytes=int(limit * 1024 * 1024)),
        cost_estimate=pl.CostEstimate(flops=int(flops), transcendentals=0, bytes_accessed=int(8e6)),
    )(*scalars, *raw, *loads)


def ring(d, along_z):
    if along_z:
        return [(z * 4 + x, ((z + d) % 4) * 4 + x) for z in range(4) for x in range(4)]
    return [(z * 4 + x, z * 4 + (x + d) % 4) for z in range(4) for x in range(4)]


def shards(block_input, value_weight, key_rows, query_rows, decay_pre, decay_log, gate_rows, out_grad):
    own = lax.axis_index("sp").astype(jnp.int32)
    own1 = own.reshape(1)
    wide, thin, half = sds((WIDE, T)), sds((STATE, T)), sds((WIDE, T), BF16)
    states, table = sds((NC, STATE, WIDE)), sds((NC, 8, C))
    DMA = pltpu.SemaphoreType.DMA
    q, k = query_rows.T, key_rows.T

    rows, gh, gl, ds, vh, vl, p1, p2, vdv, s_in, pay = staged(
        front_kernel, "front", (own1, decay_log), (block_input,), (decay_pre, q, gate_rows, out_grad, value_weight, k),
        (sds((NC, 16, C)), half, half, states, half, half, wide, wide, table, states, sds((SP, PAY, WIDE))),
        (pltpu.VMEM((2 * NC, C), F32), pltpu.VMEM((T, D), BF16), DMA((T // TT,))), 9e9, first=4,
    )
    pay_all = lax.all_to_all(pay, "sp", 0, 0, tiled=True)
    y_in, dq_in, dk_in, yg = staged(
        within_kernel, "within", (), (), (q, k, gh, gl, vh, vl), (wide, thin, thin, table), (), 3e9, limit=63.9
    )
    pay_all, yg = lax.optimization_barrier((pay_all, yg))
    pieces = staged(
        weight_kernel, "weight", (own1,), (block_input,), (pay_all, ds, rows, k, p1, p2),
        tuple(sds((4, WIDE, HALF)) for _ in range(8)),
        (pltpu.VMEM((WIDE, T), BF16), pltpu.VMEM((16, T, 256), BF16), DMA((16,))), 6e9, limit=58, keep=True,
    )
    a, b = pieces[0:4], pieces[4:8]

    z, x = own // 4, own % 4
    a_in, b_in = [], []
    for d in (1, 3, 2):
        a_in.append(lax.ppermute(a[d], "sp", ring(d, True)))
        b_in.append(lax.ppermute(b[d], "sp", ring(d, False)))
    query_grad, key_grad, decay_grad, gate_grad = staged(
        outer_kernel, "outer", (own1, decay_log), (),
        (pay_all, s_in, ds, rows, q, k, gh, gl, vh, vl, y_in, dq_in, dk_in, gate_rows, out_grad, vdv, yg, decay_pre),
        (thin, thin, sds((2, T)), sds((T, WIDE))), (pltpu.VMEM((5, 2 * NC, C), F32),), 4e9, limit=54, split=OUTER_SPLIT,
    )
    *a_in, decay_grad = lax.optimization_barrier((*a_in, decay_grad))
    a_sum = a[0] + a_in[0] + a_in[1] + a_in[2]
    b_sum = b[0] + b_in[0] + b_in[1] + b_in[2]
    piece = lambda acc, i: lax.dynamic_index_in_dim(acc, i, 0, keepdims=False)
    a_last = [piece(a_sum, x)] + [lax.ppermute(piece(a_sum, (x + d) % 4), "sp", ring(d, False)) for d in (1, 3, 2)]
    b_last = [piece(b_sum, z)] + [lax.ppermute(piece(b_sum, (z + d) % 4), "sp", ring(d, True)) for d in (1, 3, 2)]

    weight_grad, norms = pl.pallas_call(
        finish_kernel, out_shape=(sds((256, WIDE)), sds((2, HALF))), in_specs=[VMEM] * 8, out_specs=(VMEM, VMEM),
        name="finish", compiler_params=pltpu.CompilerParams(vmem_limit_bytes=4 * 1024 * 1024),
    )(*a_last, *b_last)
    norms = norms + lax.ppermute(norms, "tp", [(i, i ^ 1) for i in range(8)])
    others = [lax.ppermute(norms, "tp", [(i, (i + 2 * d) % 8) for i in range(8)]) for d in (2, 1, 3)]
    norms = norms + others[0] + others[1] + others[2]
    return key_grad.T, query_grad.T, decay_grad, gate_grad, weight_grad, norms.reshape(256)


def solution(mesh):
    in_specs = (
        P("sp", None), P(None, "tp"), P("sp", "tp"), P("sp", "tp"), P("tp", "sp"), P("tp"), P("sp", "tp"), P("sp", "tp"),
    )
    out_specs = (P("sp", "tp"), P("sp", "tp"), P("tp", "sp"), P("sp", "tp"), P("sp", "tp"), P("sp"))
    return jax.shard_map(shards, mesh=mesh, in_specs=in_specs, out_specs=out_specs, check_vma=False)
```

```python
import jax
import jax.numpy as jnp
from jax import lax
from jax.experimental import pallas as pl
from jax.experimental.pallas import tpu as pltpu
from jax.sharding import PartitionSpec as P

D = 4096
T = 2048
C = 128
NC = T // C
HEAD = 64
STATE = 64
WIDE = 128
SP = 16
PAY = 72
HALF = 128
TT = 256
PER = TT // C
F32 = jnp.float32
BF16 = jnp.bfloat16


def dot(a, b, ca=1, cb=0):
    return lax.dot_general(a, b, (((ca,), (cb,)), ((), ())), preferred_element_type=F32)


def split2(x):
    hi = x.astype(BF16)
    return hi, (x - hi.astype(F32)).astype(BF16)


def split3(x):
    hi = x.astype(BF16)
    rest = x - hi.astype(F32)
    mid = rest.astype(BF16)
    return hi, mid, (rest - mid.astype(F32)).astype(BF16)


def iota(shape, dim):
    return lax.broadcasted_iota(jnp.int32, shape, dim)


def exact_dot_r(x, ones):
    hi, mid, lo = split3(x)
    return dot(hi, ones) + dot(mid, ones) + dot(lo, ones)


def exact_dot_l(ones, x):
    hi, mid, lo = split3(x)
    return dot(ones, hi) + dot(ones, mid) + dot(ones, lo)


def ones_where(mask):
    return jnp.where(mask, 1.0, 0.0).astype(BF16)


def cat(parts, axis):
    return jnp.concatenate(parts, axis=axis)


def sigmoid(x):
    return 1.0 / (1.0 + jnp.exp(-x))


def softplus(x):
    return jnp.maximum(x, 0.0) + jnp.log(1.0 + jnp.exp(-jnp.abs(x)))


def on_lanes(row0, row1):
    return jnp.where(iota((1, WIDE), 1) < HEAD, row0, row1)


def on_rows(row0, row1):
    n = row0.shape[1]
    return jnp.where(iota((WIDE, n), 0) < HEAD, row0, row1)


def head_rows(x):
    return jnp.sum(x[:HEAD], axis=0, keepdims=True), jnp.sum(x[HEAD:], axis=0, keepdims=True)


def rates(decay_log_ref):
    odd = (iota((2 * NC, C), 0) & 1) == 1
    return jnp.exp(jnp.where(odd, decay_log_ref[1], decay_log_ref[0]))


GROW, SHRINK, WHOLE, BEFORE, AFTER = 0, 2, 4, 6, 8


def pair(rows, at):
    return rows[at : at + 1], rows[at + 1 : at + 2]


def halves(shape):
    axis = shape.index(T) if T in shape else shape.index(NC)
    n = shape[axis] // 2
    return [(slice(None),) * axis + (pl.ds(i * n, n),) for i in range(2)]


class Stage:
    def __init__(self, refs, n_scalars, n_raw, n_loads, n_outs, n_first, split):
        counts = (n_scalars, n_raw, n_loads, n_outs, n_loads, n_outs)
        groups, at = [], 0
        for n in counts:
            groups.append(refs[at : at + n])
            at += n
        self.scalars, self.raw, sources, self.targets, self.inputs, self.outs = groups
        self.in_sems, self.out_sems = refs[at], refs[at + 1]
        self.extra = refs[at + 2 :]
        self.waiting = []
        for n, (source, buffer) in enumerate(zip(sources, self.inputs)):
            self.waiting.append([
                pltpu.make_async_copy(source.at[at], buffer.at[at], self.in_sems.at[n, i])
                for i, at in enumerate(halves(buffer.shape) if n in split else [...])
            ])
        for part in range(2):
            self.begin(*range(n_first), part=part)

    def begin(self, *which, part=0):
        for n in which:
            for copy in self.waiting[n][part : part + 1]:
                copy.start()

    def load(self, *which, part=0):
        for n in which:
            for copy in self.waiting[n][part : part + 1]:
                copy.wait()
        got = [self.inputs[n] for n in which]
        return got[0] if len(got) == 1 else got

    def send(self, *which, at=None):
        for n in which:
            source, target = self.outs[n], self.targets[n]
            if at is not None:
                source, target = source.at[at], target.at[at]
            pltpu.make_async_copy(source, target, self.out_sems.at[n]).start()

    def finish(self):
        for n in range(len(self.targets)):
            pltpu.make_async_copy(self.outs[n], self.targets[n], self.out_sems.at[n]).wait()


def front_kernel(st):
    own_ref, decay_log_ref = st.scalars
    x_hbm = st.raw[0]
    flat_scr, x_scr, x_sems = st.extra
    rows_ref, gh_ref, gl_ref, ds_ref, vh_ref, vl_ref, p1_ref, p2_ref, out_rows_ref, s_ref, pay_ref = st.outs
    tiles = T // TT
    copies = []
    for n in range(tiles):
        at = pl.ds(n * TT, TT)
        copies.append(pltpu.make_async_copy(x_hbm.at[at, :], x_scr.at[at, :], x_sems.at[n]))
    for copy in copies:
        copy.start(priority=1)
    dp_ref = st.load(0)
    for c in range(NC):
        flat_scr[2 * c : 2 * c + 2, :] = dp_ref[:, c * C : (c + 1) * C]
    step = softplus(flat_scr[...])
    logs = -rates(decay_log_ref) * step
    run = exact_dot_r(logs, ones_where(iota((C, C), 0) <= iota((C, C), 1)))
    ends = jnp.broadcast_to(run[:, C - 1 : C], (2 * NC, C))
    i, j = iota((2 * NC, 2 * NC), 0), iota((2 * NC, 2 * NC), 1)
    same = (i & 1) == (j & 1)
    before = exact_dot_l(ones_where(same & (j < i)), ends)
    after = exact_dot_l(ones_where(same & (j > i)), ends)
    tables = (jnp.exp(run), jnp.exp(-run) * step, jnp.exp(ends), jnp.exp(before), jnp.exp(after))
    for c in range(NC):
        rows_ref[c] = cat([a[2 * c : 2 * c + 2] for a in tables] + [jnp.zeros((6, C), F32)], 0)
    st.send(0)
    span = jnp.exp(before[2 * NC - 2 :] + ends[2 * NC - 2 :])
    span = jnp.broadcast_to(on_lanes(span[0:1], span[1:2]), (PAY - STATE, WIDE))
    q_ref, gate_ref, og_ref, w_ref, k_ref = st.load(1, 2, 3, 4, 5)
    lower = iota((C, C), 0) <= iota((C, C), 1)

    def project(n):
        return dot(x_scr[pl.ds(pl.multiple_of(n * TT, TT), TT), :], w_ref[...]).astype(BF16)

    def chunk(c, projected, state):
        at = pl.ds(pl.multiple_of(c * C, C), C)
        pre = projected.astype(F32).T
        sig = sigmoid(pre)
        v = pre * sig
        slope = sig * (1.0 + pre * (1.0 - sig))
        rows = rows_ref[c]
        shrink = on_rows(*pair(rows, SHRINK))
        vp = v * shrink
        vh, vl = split2(vp)
        vh_ref[:, at] = vh
        vl_ref[:, at] = vl
        q, k = q_ref[:, at], k_ref[:, at]
        gate = gate_ref[at, :].astype(F32)
        g = (og_ref[at, :].astype(F32) * gate * sigmoid(gate)).T
        gh, gl = split2(g * on_rows(*pair(rows, GROW)))
        gh_ref[:, at] = gh
        gl_ref[:, at] = gl
        gg = cat([gh, gl], 1)
        ds_ref[c] = dot(cat([q, q], 1), gg, 1, 1)
        scores = jnp.where(lower, dot(k, q, 0, 0), 0.0).astype(BF16)
        dv = dot(gg, cat([scores, scores], 1), 1, 1)
        out_rows_ref[c] = cat([*head_rows(vp * dv), jnp.zeros((6, C), F32)], 0)
        turn = shrink * slope
        p1_ref[:, at] = dv * turn
        p2_ref[:, at] = turn
        s_ref[c] = state
        part = dot(cat([k, k], 1), cat([vh, vl], 1), 1, 1)
        return on_lanes(*pair(rows, WHOLE)) * (state + part)

    def process(n, projected, state):
        for m in range(PER):
            state = chunk(n * PER + m, projected[m * C : (m + 1) * C], state)
        st.send(1, 2, 4, 5, 6, 7, at=(slice(None), pl.ds(pl.multiple_of(n * TT, TT), TT)))
        return state

    def body(n, carry):
        projected, state = carry
        for i in range(1, tiles):
            @pl.when(n == i)
            def _():
                copies[i].wait()
        following = project(n)
        state = process(n - 1, projected, state)
        return following, state

    copies[0].wait()
    first = project(0)
    projected, state = lax.fori_loop(1, tiles, body, (first, jnp.zeros((STATE, WIDE), F32)))
    state = process(tiles - 1, projected, state)
    back = jnp.zeros((STATE, WIDE), F32)
    for c in range(NC - 1, -1, -1):
        part = ds_ref[c]
        ds_ref[c] = back
        back = part + on_lanes(*pair(rows_ref[c], WHOLE)) * back
    own = own_ref[0]
    for n in range(SP):
        pay_ref[n] = cat([jnp.where(n > own, state, back), span], 0)
    st.send(10, 3, 8, 9)


def within_kernel(st):
    q_ref, k_ref, gh_ref, gl_ref, vh_ref, vl_ref = st.load(0, 1, 2, 3, 4, 5)
    y_ref, dq_ref, dk_ref, out_rows_ref = st.outs
    lower = iota((C, C), 0) <= iota((C, C), 1)

    def chunk(c, carry):
        at = pl.ds(pl.multiple_of(c * C, C), C)
        q, k = q_ref[:, at], k_ref[:, at]
        gh, gl, vh, vl = gh_ref[:, at], gl_ref[:, at], vh_ref[:, at], vl_ref[:, at]
        scores = jnp.where(lower, dot(k, q, 0, 0), 0.0).astype(BF16)
        y = dot(cat([vh, vl], 1), cat([scores, scores], 0))
        prods = dot(cat([vh, vh], 0), cat([gh, gl], 0), 0, 0) + dot(vl, gh, 0, 0)
        ph, plo = split2(jnp.where(lower, prods, 0.0))
        y_ref[:, at] = y
        dq_ref[:, at] = dot(cat([k, k], 1), cat([ph, plo], 0))
        dk_ref[:, at] = dot(cat([q, q], 1), cat([ph, plo], 1), 1, 1)
        yg = head_rows(y * (gh.astype(F32) + gl.astype(F32)))
        out_rows_ref[c] = cat([*yg, jnp.zeros((6, C), F32)], 0)
        st.send(0, 1, 2, at=(slice(None), at))
        return carry

    lax.fori_loop(0, NC, chunk, 0, unroll=UNROLL)
    st.send(3)


def suffix_state(own, pay_ref):
    acc = jnp.zeros((STATE, WIDE), F32)
    for j in range(SP - 1, 0, -1):
        acc = jnp.where(j > own, pay_ref[j, :STATE, :] + pay_ref[j, STATE : STATE + 1, :] * acc, acc)
    return acc


def prefix_state(own, pay_ref):
    acc = jnp.zeros((STATE, WIDE), F32)
    for j in range(SP - 1):
        acc = jnp.where(j < own, pay_ref[j, :STATE, :] + pay_ref[j, STATE : STATE + 1, :] * acc, acc)
    return acc


ORDER = (1, 3, 2, 0)


def weight_kernel(st):
    own = st.scalars[0][0]
    x_hbm = st.raw[0]
    vg_scr, x_scr, x_sems = st.extra
    z, x = own // 4, own % 4
    tiles = []
    for dz in ORDER:
        for pair_of in (ORDER[:2], ORDER[2:]):
            n, parts = len(tiles), []
            for m, dx in enumerate(pair_of):
                oz, ox = (z + dz) % 4, (x + dx) % 4
                at = pl.ds(pl.multiple_of((oz * 4 + ox) * 256, 256), 256)
                copy = pltpu.make_async_copy(x_hbm.at[:, at], x_scr.at[n, :, pl.ds(m * 256, 256)], x_sems.at[n, m])
                copy.start(priority=1)
                parts.append((copy, dx, oz, ox))
            tiles.append((dz, parts))
    pay_ref, ds_ref, rows_ref, k_ref, p1_ref, p2_ref = st.load(0, 1, 2, 3, 4, 5)
    outgoing = suffix_state(own, pay_ref)
    for c in range(NC):
        at = slice(c * C, (c + 1) * C)
        rows = rows_ref[c]
        back = on_lanes(*pair(rows, WHOLE)) * (ds_ref[c] + on_lanes(*pair(rows, AFTER)) * outgoing)
        k = k_ref[:, at]
        carried = dot(cat(split2(back), 0), cat([k, k], 0), 0, 0)
        vg_scr[:, at] = (p1_ref[:, at] + p2_ref[:, at] * carried).astype(BF16)
    for n, (dz, parts) in enumerate(tiles):
        for copy, *_ in parts:
            copy.wait()
        part = dot(vg_scr[...], x_scr[n])
        for m, (_, dx, oz, ox) in enumerate(parts):
            st.outs[dz][ox] = part[:, m * 256 : m * 256 + HALF]
            st.outs[4 + dx][oz] = part[:, m * 256 + HALF : (m + 1) * 256]
            st.send(dz, at=ox)
            st.send(4 + dx, at=oz)


def outer_kernel(st):
    own_ref, decay_log_ref = st.scalars
    flat_scr = st.extra[0]
    (pay_ref, s_ref, ds_ref, rows_ref, q_ref, k_ref, gh_ref, gl_ref, vh_ref, vl_ref, y_ref, dq_ref, dk_ref,
     gate_ref, og_ref, vdv_ref, yg_ref, dp_ref) = st.load(*range(18))
    dq_out, dk_out, decay_out, gate_out = st.outs
    incoming = prefix_state(own_ref[0], pay_ref)
    outgoing = suffix_state(own_ref[0], pay_ref)

    def chunk(c, carry):
        at = pl.ds(pl.multiple_of(c * C, C), C)
        rows = rows_ref[c]
        state = s_ref[c] + on_lanes(*pair(rows, BEFORE)) * incoming
        back = on_lanes(*pair(rows, WHOLE)) * (ds_ref[c] + on_lanes(*pair(rows, AFTER)) * outgoing)
        sh, sl = split2(state)
        bh, bl = split2(back)
        q, k = q_ref[:, at], k_ref[:, at]
        gh, gl, vh, vl = gh_ref[:, at], gl_ref[:, at], vh_ref[:, at], vl_ref[:, at]
        yo = dot(cat([sh, sl], 0), cat([q, q], 0), 0, 0)
        vo = dot(cat([bh, bl], 0), cat([k, k], 0), 0, 0)
        y = ((y_ref[:, at] + yo) * on_rows(*pair(rows, GROW))).T
        gate = gate_ref[at, :].astype(F32)
        sg = sigmoid(gate)
        gate_out[at, :] = og_ref[at, :].astype(F32) * y * sg * (1.0 + gate * (1.0 - sg))
        dq_out[:, at] = dq_ref[:, at] + dot(cat([sh, sh, sl], 1), cat([gh, gl, gh], 0))
        dk_out[:, at] = dk_ref[:, at] + dot(cat([bh, bh, bl], 1), cat([vh, vl, vh], 0))
        yg = head_rows(yo * (gh.astype(F32) + gl.astype(F32)))
        cs = head_rows(vo * (vh.astype(F32) + vl.astype(F32)))
        through = jnp.sum(state * back, axis=0, keepdims=True)
        first = iota((1, WIDE), 1) < HEAD
        vdv = vdv_ref[c, 0:2, :]
        p = pl.ds(2 * c, 2)
        flat_scr[0, p, :] = cat(yg, 0) + yg_ref[c, 0:2, :] - vdv
        flat_scr[1, p, :] = cat(cs, 0)
        flat_scr[2, p, :] = cat([jnp.where(first, through, 0.0), jnp.where(first, 0.0, through)], 0)
        flat_scr[3, p, :] = vdv
        st.send(0, 1, at=(slice(None), at))
        st.send(3, at=(at, slice(None)))
        return carry

    lax.fori_loop(0, NC // 2, chunk, 0, unroll=UNROLL)
    st.load(*OUTER_SPLIT, part=1)
    lax.fori_loop(NC // 2, NC, chunk, 0, unroll=UNROLL)
    for c in range(NC):
        flat_scr[4, 2 * c : 2 * c + 2, :] = dp_ref[:, c * C : (c + 1) * C]
    t, s = iota((C, C), 0), iota((C, C), 1)
    cs = flat_scr[1]
    log_back = (
        exact_dot_r(flat_scr[0], ones_where(t >= s))
        + exact_dot_r(cs, ones_where(t < s))
        + exact_dot_r(flat_scr[2], jnp.ones((C, C), BF16))
    )
    dp = flat_scr[4]
    size_back = (flat_scr[3] + cs) / softplus(dp)
    flat_scr[0] = (size_back - rates(decay_log_ref) * log_back) * sigmoid(dp)
    for c in range(NC):
        decay_out[:, c * C : (c + 1) * C] = flat_scr[0, 2 * c : 2 * c + 2, :]
    st.send(2)


UNROLL = 8
OUTER_SPLIT = (1, 2, 4, 5, 6, 7, 8, 9, 10, 11, 12, 13, 14)


def finish_kernel(*refs):
    a_refs, b_refs, w_ref, n_ref = refs[0:4], refs[4:8], refs[8], refs[9]
    a = a_refs[0][...] + a_refs[1][...] + a_refs[2][...] + a_refs[3][...]
    b = b_refs[0][...] + b_refs[1][...] + b_refs[2][...] + b_refs[3][...]
    w_ref[:HALF, :] = a.T
    w_ref[HALF:, :] = b.T
    n_ref[0:1, :] = jnp.sum(a * a, axis=0, keepdims=True)
    n_ref[1:2, :] = jnp.sum(b * b, axis=0, keepdims=True)


def sds(shape, dtype=F32):
    return jax.ShapeDtypeStruct(shape, dtype)


SMEM = pl.BlockSpec(memory_space=pltpu.SMEM)
VMEM = pl.BlockSpec(memory_space=pltpu.VMEM)
HBM = pl.BlockSpec(memory_space=pl.ANY)


def staged(kernel, name, scalars, raw, loads, outs, extra=(), flops=1e9, limit=62, first=None, keep=False, split=()):
    first = len(loads) if first is None else first

    def wrapped(*refs):
        if keep:
            at = len(scalars) + len(raw) + len(loads)
            kept, n = refs[at : at + len(outs)], len(loads)
            refs = refs[:at] + refs[at + len(outs) :]
            st = Stage(refs, len(scalars), len(raw), n, 0, first, split)
            st.outs = kept
        else:
            st = Stage(refs, len(scalars), len(raw), len(loads), len(outs), first, split)
        kernel(st)
        st.finish()

    DMA = pltpu.SemaphoreType.DMA
    return pl.pallas_call(
        wrapped, out_shape=tuple(outs), out_specs=tuple([VMEM if keep else HBM] * len(outs)),
        in_specs=[SMEM] * len(scalars) + [HBM] * (len(raw) + len(loads)), name=name,
        scratch_shapes=[pltpu.VMEM(a.shape, a.dtype) for a in (*loads, *(() if keep else outs))]
        + [DMA((max(len(loads), 1), 2)), DMA((len(outs),)), *extra],
        compiler_params=pltpu.CompilerParams(vmem_limit_bytes=int(limit * 1024 * 1024)),
        cost_estimate=pl.CostEstimate(flops=int(flops), transcendentals=0, bytes_accessed=int(8e6)),
    )(*scalars, *raw, *loads)


def ring(d, along_z):
    if along_z:
        return [(z * 4 + x, ((z + d) % 4) * 4 + x) for z in range(4) for x in range(4)]
    return [(z * 4 + x, z * 4 + (x + d) % 4) for z in range(4) for x in range(4)]


def shards(block_input, value_weight, key_rows, query_rows, decay_pre, decay_log, gate_rows, out_grad):
    own = lax.axis_index("sp").astype(jnp.int32)
    own1 = own.reshape(1)
    wide, thin, half = sds((WIDE, T)), sds((STATE, T)), sds((WIDE, T), BF16)
    states, table = sds((NC, STATE, WIDE)), sds((NC, 8, C))
    DMA = pltpu.SemaphoreType.DMA
    q, k = query_rows.T, key_rows.T

    rows, gh, gl, ds, vh, vl, p1, p2, vdv, s_in, pay = staged(
        front_kernel, "front", (own1, decay_log), (block_input,), (decay_pre, q, gate_rows, out_grad, value_weight, k),
        (sds((NC, 16, C)), half, half, states, half, half, wide, wide, table, states, sds((SP, PAY, WIDE))),
        (pltpu.VMEM((2 * NC, C), F32), pltpu.VMEM((T, D), BF16), DMA((T // TT,))), 9e9,
    )
    pay_all = lax.all_to_all(pay, "sp", 0, 0, tiled=True)
    y_in, dq_in, dk_in, yg = staged(
        within_kernel, "within", (), (), (q, k, gh, gl, vh, vl), (wide, thin, thin, table), (), 3e9, limit=63.9
    )
    pay_all, yg = lax.optimization_barrier((pay_all, yg))
    pieces = staged(
        weight_kernel, "weight", (own1,), (block_input,), (pay_all, ds, rows, k, p1, p2),
        tuple(sds((4, WIDE, HALF)) for _ in range(8)),
        (pltpu.VMEM((WIDE, T), BF16), pltpu.VMEM((8, T, 512), BF16), DMA((8, 2))), 6e9,
    )
    a, b = pieces[0:4], pieces[4:8]

    z, x = own // 4, own % 4
    a_in, b_in = [], []
    for d in (1, 3, 2):
        a_in.append(lax.ppermute(a[d], "sp", ring(d, True)))
        b_in.append(lax.ppermute(b[d], "sp", ring(d, False)))
    query_grad, key_grad, decay_grad, gate_grad = staged(
        outer_kernel, "outer", (own1, decay_log), (),
        (pay_all, s_in, ds, rows, q, k, gh, gl, vh, vl, y_in, dq_in, dk_in, gate_rows, out_grad, vdv, yg, decay_pre),
        (thin, thin, sds((2, T)), sds((T, WIDE))), (pltpu.VMEM((5, 2 * NC, C), F32),), 4e9, limit=54, split=OUTER_SPLIT,
    )
    *a_in, decay_grad = lax.optimization_barrier((*a_in, decay_grad))
    a_sum = a[0] + a_in[0] + a_in[1] + a_in[2]
    b_sum = b[0] + b_in[0] + b_in[1] + b_in[2]
    piece = lambda acc, i: lax.dynamic_index_in_dim(acc, i, 0, keepdims=False)
    a_last = [piece(a_sum, x)] + [lax.ppermute(piece(a_sum, (x + d) % 4), "sp", ring(d, False)) for d in (1, 3, 2)]
    b_last = [piece(b_sum, z)] + [lax.ppermute(piece(b_sum, (z + d) % 4), "sp", ring(d, True)) for d in (1, 3, 2)]

    weight_grad, norms = pl.pallas_call(
        finish_kernel, out_shape=(sds((256, WIDE)), sds((2, HALF))), in_specs=[VMEM] * 8, out_specs=(VMEM, VMEM),
        name="finish", compiler_params=pltpu.CompilerParams(vmem_limit_bytes=4 * 1024 * 1024),
    )(*a_last, *b_last)
    norms = norms + lax.ppermute(norms, "tp", [(i, i ^ 1) for i in range(8)])
    others = [lax.ppermute(norms, "tp", [(i, (i + 2 * d) % 8) for i in range(8)]) for d in (2, 1, 3)]
    norms = norms + others[0] + others[1] + others[2]
    return key_grad.T, query_grad.T, decay_grad, gate_grad, weight_grad, norms.reshape(256)


def solution(mesh):
    in_specs = (
        P("sp", None), P(None, "tp"), P("sp", "tp"), P("sp", "tp"), P("tp", "sp"), P("tp"), P("sp", "tp"), P("sp", "tp"),
    )
    out_specs = (P("sp", "tp"), P("sp", "tp"), P("tp", "sp"), P("sp", "tp"), P("sp", "tp"), P("sp"))
    return jax.shard_map(shards, mesh=mesh, in_specs=in_specs, out_specs=out_specs, check_vma=False)
```

```python
import jax
import jax.numpy as jnp
from jax import lax
from jax.experimental import pallas as pl
from jax.experimental.pallas import tpu as pltpu
from jax.sharding import PartitionSpec as P

D = 4096
T = 2048
C = 128
NC = T // C
HEAD = 64
STATE = 64
WIDE = 128
SP = 16
PAY = 72
HALF = 128
TT = 256
PER = TT // C
F32 = jnp.float32
BF16 = jnp.bfloat16


def dot(a, b, ca=1, cb=0):
    return lax.dot_general(a, b, (((ca,), (cb,)), ((), ())), preferred_element_type=F32)


def split2(x):
    hi = x.astype(BF16)
    return hi, (x - hi.astype(F32)).astype(BF16)


def split3(x):
    hi = x.astype(BF16)
    rest = x - hi.astype(F32)
    mid = rest.astype(BF16)
    return hi, mid, (rest - mid.astype(F32)).astype(BF16)


def iota(shape, dim):
    return lax.broadcasted_iota(jnp.int32, shape, dim)


def exact_dot_r(x, ones):
    hi, mid, lo = split3(x)
    return dot(hi, ones) + dot(mid, ones) + dot(lo, ones)


def exact_dot_l(ones, x):
    hi, mid, lo = split3(x)
    return dot(ones, hi) + dot(ones, mid) + dot(ones, lo)


def ones_where(mask):
    return jnp.where(mask, 1.0, 0.0).astype(BF16)


def cat(parts, axis):
    return jnp.concatenate(parts, axis=axis)


def sigmoid(x):
    return 1.0 / (1.0 + jnp.exp(-x))


def softplus(x):
    return jnp.maximum(x, 0.0) + jnp.log(1.0 + jnp.exp(-jnp.abs(x)))


def on_lanes(row0, row1):
    return jnp.where(iota((1, WIDE), 1) < HEAD, row0, row1)


def on_rows(row0, row1):
    n = row0.shape[1]
    return jnp.where(iota((WIDE, n), 0) < HEAD, row0, row1)


def head_rows(x):
    return jnp.sum(x[:HEAD], axis=0, keepdims=True), jnp.sum(x[HEAD:], axis=0, keepdims=True)


def rates(decay_log_ref):
    odd = (iota((2 * NC, C), 0) & 1) == 1
    return jnp.exp(jnp.where(odd, decay_log_ref[1], decay_log_ref[0]))


GROW, SHRINK, WHOLE, BEFORE, AFTER = 0, 2, 4, 6, 8


def pair(rows, at):
    return rows[at : at + 1], rows[at + 1 : at + 2]


def halves(shape):
    axis = shape.index(T) if T in shape else shape.index(NC)
    n = shape[axis] // 2
    return [(slice(None),) * axis + (pl.ds(i * n, n),) for i in range(2)]


class Stage:
    def __init__(self, refs, n_scalars, n_raw, n_loads, n_outs, n_first, split):
        counts = (n_scalars, n_raw, n_loads, n_outs, n_loads, n_outs)
        groups, at = [], 0
        for n in counts:
            groups.append(refs[at : at + n])
            at += n
        self.scalars, self.raw, sources, self.targets, self.inputs, self.outs = groups
        self.in_sems, self.out_sems = refs[at], refs[at + 1]
        self.extra = refs[at + 2 :]
        self.waiting = []
        for n, (source, buffer) in enumerate(zip(sources, self.inputs)):
            self.waiting.append([
                pltpu.make_async_copy(source.at[at], buffer.at[at], self.in_sems.at[n, i])
                for i, at in enumerate(halves(buffer.shape) if n in split else [...])
            ])
        for part in range(2):
            self.begin(*range(n_first), part=part)

    def begin(self, *which, part=0):
        for n in which:
            for copy in self.waiting[n][part : part + 1]:
                copy.start()

    def load(self, *which, part=0):
        for n in which:
            for copy in self.waiting[n][part : part + 1]:
                copy.wait()
        got = [self.inputs[n] for n in which]
        return got[0] if len(got) == 1 else got

    def send(self, *which, at=None):
        for n in which:
            source, target = self.outs[n], self.targets[n]
            if at is not None:
                source, target = source.at[at], target.at[at]
            pltpu.make_async_copy(source, target, self.out_sems.at[n]).start()

    def finish(self):
        for n in range(len(self.targets)):
            pltpu.make_async_copy(self.outs[n], self.targets[n], self.out_sems.at[n]).wait()


def front_kernel(st):
    own_ref, decay_log_ref = st.scalars
    x_hbm = st.raw[0]
    flat_scr, x_scr, x_sems = st.extra
    rows_ref, gh_ref, gl_ref, ds_ref, vh_ref, vl_ref, p1_ref, p2_ref, out_rows_ref, s_ref, pay_ref = st.outs
    tiles = T // TT
    copies = []
    for n in range(tiles):
        at = pl.ds(n * TT, TT)
        copies.append(pltpu.make_async_copy(x_hbm.at[at, :], x_scr.at[at, :], x_sems.at[n]))
    for copy in copies:
        copy.start(priority=1)
    dp_ref = st.load(0)
    for c in range(NC):
        flat_scr[2 * c : 2 * c + 2, :] = dp_ref[:, c * C : (c + 1) * C]
    step = softplus(flat_scr[...])
    logs = -rates(decay_log_ref) * step
    run = exact_dot_r(logs, ones_where(iota((C, C), 0) <= iota((C, C), 1)))
    ends = jnp.broadcast_to(run[:, C - 1 : C], (2 * NC, C))
    i, j = iota((2 * NC, 2 * NC), 0), iota((2 * NC, 2 * NC), 1)
    same = (i & 1) == (j & 1)
    before = exact_dot_l(ones_where(same & (j < i)), ends)
    after = exact_dot_l(ones_where(same & (j > i)), ends)
    tables = (jnp.exp(run), jnp.exp(-run) * step, jnp.exp(ends), jnp.exp(before), jnp.exp(after))
    for c in range(NC):
        rows_ref[c] = cat([a[2 * c : 2 * c + 2] for a in tables] + [jnp.zeros((6, C), F32)], 0)
    st.send(0)
    span = jnp.exp(before[2 * NC - 2 :] + ends[2 * NC - 2 :])
    span = jnp.broadcast_to(on_lanes(span[0:1], span[1:2]), (PAY - STATE, WIDE))
    w_ref = st.load(4)
    q_ref, gate_ref, og_ref, k_ref = (st.inputs[n] for n in (1, 2, 3, 5))
    lower = iota((C, C), 0) <= iota((C, C), 1)

    def project(n):
        return dot(x_scr[pl.ds(pl.multiple_of(n * TT, TT), TT), :], w_ref[...]).astype(BF16)

    def chunk(c, projected, state):
        at = pl.ds(pl.multiple_of(c * C, C), C)
        pre = projected.astype(F32).T
        sig = sigmoid(pre)
        v = pre * sig
        slope = sig * (1.0 + pre * (1.0 - sig))
        rows = rows_ref[c]
        shrink = on_rows(*pair(rows, SHRINK))
        vp = v * shrink
        vh, vl = split2(vp)
        vh_ref[:, at] = vh
        vl_ref[:, at] = vl
        q, k = q_ref[:, at], k_ref[:, at]
        gate = gate_ref[at, :].astype(F32)
        g = (og_ref[at, :].astype(F32) * gate * sigmoid(gate)).T
        gh, gl = split2(g * on_rows(*pair(rows, GROW)))
        gh_ref[:, at] = gh
        gl_ref[:, at] = gl
        gg = cat([gh, gl], 1)
        ds_ref[c] = dot(cat([q, q], 1), gg, 1, 1)
        scores = jnp.where(lower, dot(k, q, 0, 0), 0.0).astype(BF16)
        dv = dot(gg, cat([scores, scores], 1), 1, 1)
        out_rows_ref[c] = cat([*head_rows(vp * dv), jnp.zeros((6, C), F32)], 0)
        turn = shrink * slope
        p1_ref[:, at] = dv * turn
        p2_ref[:, at] = turn
        s_ref[c] = state
        part = dot(cat([k, k], 1), cat([vh, vl], 1), 1, 1)
        return on_lanes(*pair(rows, WHOLE)) * (state + part)

    def process(n, projected, state):
        for m in range(PER):
            state = chunk(n * PER + m, projected[m * C : (m + 1) * C], state)
        st.send(1, 2, 4, 5, 6, 7, at=(slice(None), pl.ds(pl.multiple_of(n * TT, TT), TT)))
        st.send(8, 9, at=pl.ds(n * PER, PER))
        return state

    def body(n, carry):
        projected, state = carry
        for i in range(1, tiles):
            @pl.when(n == i)
            def _():
                copies[i].wait()
        following = project(n)
        state = process(n - 1, projected, state)
        return following, state

    copies[0].wait()
    first = project(0)
    st.load(1, 2, 3, 5)
    projected, state = lax.fori_loop(1, tiles, body, (first, jnp.zeros((STATE, WIDE), F32)))
    state = process(tiles - 1, projected, state)
    back = jnp.zeros((STATE, WIDE), F32)
    for c in range(NC - 1, -1, -1):
        part = ds_ref[c]
        ds_ref[c] = back
        back = part + on_lanes(*pair(rows_ref[c], WHOLE)) * back
    own = own_ref[0]
    for n in range(SP):
        pay_ref[n] = cat([jnp.where(n > own, state, back), span], 0)
    st.send(10, 3)


def within_kernel(st):
    q_ref, k_ref, gh_ref, gl_ref, vh_ref, vl_ref = st.load(0, 1, 2, 3, 4, 5)
    y_ref, dq_ref, dk_ref, out_rows_ref = st.outs
    lower = iota((C, C), 0) <= iota((C, C), 1)

    def chunk(c, carry):
        at = pl.ds(pl.multiple_of(c * C, C), C)
        q, k = q_ref[:, at], k_ref[:, at]
        gh, gl, vh, vl = gh_ref[:, at], gl_ref[:, at], vh_ref[:, at], vl_ref[:, at]
        scores = jnp.where(lower, dot(k, q, 0, 0), 0.0).astype(BF16)
        y = dot(cat([vh, vl], 1), cat([scores, scores], 0))
        prods = dot(cat([vh, vh], 0), cat([gh, gl], 0), 0, 0) + dot(vl, gh, 0, 0)
        ph, plo = split2(jnp.where(lower, prods, 0.0))
        y_ref[:, at] = y
        dq_ref[:, at] = dot(cat([k, k], 1), cat([ph, plo], 0))
        dk_ref[:, at] = dot(cat([q, q], 1), cat([ph, plo], 1), 1, 1)
        yg = head_rows(y * (gh.astype(F32) + gl.astype(F32)))
        out_rows_ref[c] = cat([*yg, jnp.zeros((6, C), F32)], 0)
        st.send(0, 1, 2, at=(slice(None), at))
        return carry

    lax.fori_loop(0, NC, chunk, 0, unroll=UNROLL)
    st.send(3)


def suffix_state(own, pay_ref):
    acc = jnp.zeros((STATE, WIDE), F32)
    for j in range(SP - 1, 0, -1):
        acc = jnp.where(j > own, pay_ref[j, :STATE, :] + pay_ref[j, STATE : STATE + 1, :] * acc, acc)
    return acc


def prefix_state(own, pay_ref):
    acc = jnp.zeros((STATE, WIDE), F32)
    for j in range(SP - 1):
        acc = jnp.where(j < own, pay_ref[j, :STATE, :] + pay_ref[j, STATE : STATE + 1, :] * acc, acc)
    return acc


ORDER = (1, 3, 2, 0)


def weight_kernel(st):
    own = st.scalars[0][0]
    x_hbm = st.raw[0]
    vg_scr, x_scr, x_sems = st.extra
    z, x = own // 4, own % 4
    tiles = []
    for dz in ORDER:
        for pair_of in (ORDER[:2], ORDER[2:]):
            n, parts = len(tiles), []
            for m, dx in enumerate(pair_of):
                oz, ox = (z + dz) % 4, (x + dx) % 4
                at = pl.ds(pl.multiple_of((oz * 4 + ox) * 256, 256), 256)
                copy = pltpu.make_async_copy(x_hbm.at[:, at], x_scr.at[n, :, pl.ds(m * 256, 256)], x_sems.at[n, m])
                copy.start(priority=1)
                parts.append((copy, dx, oz, ox))
            tiles.append((dz, parts))
    pay_ref, ds_ref, rows_ref, k_ref, p1_ref, p2_ref = st.load(0, 1, 2, 3, 4, 5)
    outgoing = suffix_state(own, pay_ref)
    for c in range(NC):
        if c == NC // 2:
            st.load(*WEIGHT_SPLIT, part=1)
        at = slice(c * C, (c + 1) * C)
        rows = rows_ref[c]
        back = on_lanes(*pair(rows, WHOLE)) * (ds_ref[c] + on_lanes(*pair(rows, AFTER)) * outgoing)
        k = k_ref[:, at]
        carried = dot(cat(split2(back), 0), cat([k, k], 0), 0, 0)
        vg_scr[:, at] = (p1_ref[:, at] + p2_ref[:, at] * carried).astype(BF16)
    for n, (dz, parts) in enumerate(tiles):
        for copy, *_ in parts:
            copy.wait()
        part = dot(vg_scr[...], x_scr[n])
        for m, (_, dx, oz, ox) in enumerate(parts):
            st.outs[dz][ox] = part[:, m * 256 : m * 256 + HALF]
            st.outs[4 + dx][oz] = part[:, m * 256 + HALF : (m + 1) * 256]
            st.send(dz, at=ox)
            st.send(4 + dx, at=oz)


def outer_kernel(st):
    own_ref, decay_log_ref = st.scalars
    flat_scr = st.extra[0]
    (pay_ref, s_ref, ds_ref, rows_ref, q_ref, k_ref, gh_ref, gl_ref, vh_ref, vl_ref, y_ref, dq_ref, dk_ref,
     gate_ref, og_ref, vdv_ref, yg_ref, dp_ref) = st.load(*range(18))
    dq_out, dk_out, decay_out, gate_out = st.outs
    incoming = prefix_state(own_ref[0], pay_ref)
    outgoing = suffix_state(own_ref[0], pay_ref)

    def chunk(c, carry):
        at = pl.ds(pl.multiple_of(c * C, C), C)
        rows = rows_ref[c]
        state = s_ref[c] + on_lanes(*pair(rows, BEFORE)) * incoming
        back = on_lanes(*pair(rows, WHOLE)) * (ds_ref[c] + on_lanes(*pair(rows, AFTER)) * outgoing)
        sh, sl = split2(state)
        bh, bl = split2(back)
        q, k = q_ref[:, at], k_ref[:, at]
        gh, gl, vh, vl = gh_ref[:, at], gl_ref[:, at], vh_ref[:, at], vl_ref[:, at]
        yo = dot(cat([sh, sl], 0), cat([q, q], 0), 0, 0)
        vo = dot(cat([bh, bl], 0), cat([k, k], 0), 0, 0)
        y = ((y_ref[:, at] + yo) * on_rows(*pair(rows, GROW))).T
        gate = gate_ref[at, :].astype(F32)
        sg = sigmoid(gate)
        gate_out[at, :] = og_ref[at, :].astype(F32) * y * sg * (1.0 + gate * (1.0 - sg))
        dq_out[:, at] = dq_ref[:, at] + dot(cat([sh, sh, sl], 1), cat([gh, gl, gh], 0))
        dk_out[:, at] = dk_ref[:, at] + dot(cat([bh, bh, bl], 1), cat([vh, vl, vh], 0))
        yg = head_rows(yo * (gh.astype(F32) + gl.astype(F32)))
        cs = head_rows(vo * (vh.astype(F32) + vl.astype(F32)))
        through = jnp.sum(state * back, axis=0, keepdims=True)
        first = iota((1, WIDE), 1) < HEAD
        vdv = vdv_ref[c, 0:2, :]
        p = pl.ds(2 * c, 2)
        flat_scr[0, p, :] = cat(yg, 0) + yg_ref[c, 0:2, :] - vdv
        flat_scr[1, p, :] = cat(cs, 0)
        flat_scr[2, p, :] = cat([jnp.where(first, through, 0.0), jnp.where(first, 0.0, through)], 0)
        flat_scr[3, p, :] = vdv
        st.send(0, 1, at=(slice(None), at))
        st.send(3, at=(at, slice(None)))
        return carry

    lax.fori_loop(0, NC // 2, chunk, 0, unroll=UNROLL)
    st.load(*OUTER_SPLIT, part=1)
    lax.fori_loop(NC // 2, NC, chunk, 0, unroll=UNROLL)
    for c in range(NC):
        flat_scr[4, 2 * c : 2 * c + 2, :] = dp_ref[:, c * C : (c + 1) * C]
    t, s = iota((C, C), 0), iota((C, C), 1)
    cs = flat_scr[1]
    log_back = (
        exact_dot_r(flat_scr[0], ones_where(t >= s))
        + exact_dot_r(cs, ones_where(t < s))
        + exact_dot_r(flat_scr[2], jnp.ones((C, C), BF16))
    )
    dp = flat_scr[4]
    size_back = (flat_scr[3] + cs) / softplus(dp)
    flat_scr[0] = (size_back - rates(decay_log_ref) * log_back) * sigmoid(dp)
    for c in range(NC):
        decay_out[:, c * C : (c + 1) * C] = flat_scr[0, 2 * c : 2 * c + 2, :]
    st.send(2)


UNROLL = 8
WEIGHT_SPLIT = (1, 4, 5)
OUTER_SPLIT = (1, 2, 4, 5, 6, 7, 8, 9, 10, 11, 12, 13, 14)


def finish_kernel(*refs):
    a_refs, b_refs, w_ref, n_ref = refs[0:4], refs[4:8], refs[8], refs[9]
    a = a_refs[0][...] + a_refs[1][...] + a_refs[2][...] + a_refs[3][...]
    b = b_refs[0][...] + b_refs[1][...] + b_refs[2][...] + b_refs[3][...]
    w_ref[:HALF, :] = a.T
    w_ref[HALF:, :] = b.T
    n_ref[0:1, :] = jnp.sum(a * a, axis=0, keepdims=True)
    n_ref[1:2, :] = jnp.sum(b * b, axis=0, keepdims=True)


def sds(shape, dtype=F32):
    return jax.ShapeDtypeStruct(shape, dtype)


SMEM = pl.BlockSpec(memory_space=pltpu.SMEM)
VMEM = pl.BlockSpec(memory_space=pltpu.VMEM)
HBM = pl.BlockSpec(memory_space=pl.ANY)


def staged(kernel, name, scalars, raw, loads, outs, extra=(), flops=1e9, limit=62, first=None, keep=False, split=()):
    first = len(loads) if first is None else first

    def wrapped(*refs):
        if keep:
            at = len(scalars) + len(raw) + len(loads)
            kept, n = refs[at : at + len(outs)], len(loads)
            refs = refs[:at] + refs[at + len(outs) :]
            st = Stage(refs, len(scalars), len(raw), n, 0, first, split)
            st.outs = kept
        else:
            st = Stage(refs, len(scalars), len(raw), len(loads), len(outs), first, split)
        kernel(st)
        st.finish()

    DMA = pltpu.SemaphoreType.DMA
    return pl.pallas_call(
        wrapped, out_shape=tuple(outs), out_specs=tuple([VMEM if keep else HBM] * len(outs)),
        in_specs=[SMEM] * len(scalars) + [HBM] * (len(raw) + len(loads)), name=name,
        scratch_shapes=[pltpu.VMEM(a.shape, a.dtype) for a in (*loads, *(() if keep else outs))]
        + [DMA((max(len(loads), 1), 2)), DMA((len(outs),)), *extra],
        compiler_params=pltpu.CompilerParams(vmem_limit_bytes=int(limit * 1024 * 1024)),
        cost_estimate=pl.CostEstimate(flops=int(flops), transcendentals=0, bytes_accessed=int(8e6)),
    )(*scalars, *raw, *loads)


def ring(d, along_z):
    if along_z:
        return [(z * 4 + x, ((z + d) % 4) * 4 + x) for z in range(4) for x in range(4)]
    return [(z * 4 + x, z * 4 + (x + d) % 4) for z in range(4) for x in range(4)]


def shards(block_input, value_weight, key_rows, query_rows, decay_pre, decay_log, gate_rows, out_grad):
    own = lax.axis_index("sp").astype(jnp.int32)
    own1 = own.reshape(1)
    wide, thin, half = sds((WIDE, T)), sds((STATE, T)), sds((WIDE, T), BF16)
    states, table = sds((NC, STATE, WIDE)), sds((NC, 8, C))
    DMA = pltpu.SemaphoreType.DMA
    q, k = query_rows.T, key_rows.T

    rows, gh, gl, ds, vh, vl, p1, p2, vdv, s_in, pay = staged(
        front_kernel, "front", (own1, decay_log), (block_input,), (decay_pre, q, gate_rows, out_grad, value_weight, k),
        (sds((NC, 16, C)), half, half, states, half, half, wide, wide, table, states, sds((SP, PAY, WIDE))),
        (pltpu.VMEM((2 * NC, C), F32), pltpu.VMEM((T, D), BF16), DMA((T // TT,))), 9e9,
    )
    pay_all = lax.all_to_all(pay, "sp", 0, 0, tiled=True)
    y_in, dq_in, dk_in, yg = staged(
        within_kernel, "within", (), (), (q, k, gh, gl, vh, vl), (wide, thin, thin, table), (), 3e9, limit=63.9
    )
    pay_all, yg = lax.optimization_barrier((pay_all, yg))
    pieces = staged(
        weight_kernel, "weight", (own1,), (block_input,), (pay_all, ds, rows, k, p1, p2),
        tuple(sds((4, WIDE, HALF)) for _ in range(8)),
        (pltpu.VMEM((WIDE, T), BF16), pltpu.VMEM((8, T, 512), BF16), DMA((8, 2))), 6e9, split=WEIGHT_SPLIT,
    )
    a, b = pieces[0:4], pieces[4:8]

    z, x = own // 4, own % 4
    a_in, b_in = [], []
    for d in (1, 3, 2):
        a_in.append(lax.ppermute(a[d], "sp", ring(d, True)))
        b_in.append(lax.ppermute(b[d], "sp", ring(d, False)))
    query_grad, key_grad, decay_grad, gate_grad = staged(
        outer_kernel, "outer", (own1, decay_log), (),
        (pay_all, s_in, ds, rows, q, k, gh, gl, vh, vl, y_in, dq_in, dk_in, gate_rows, out_grad, vdv, yg, decay_pre),
        (thin, thin, sds((2, T)), sds((T, WIDE))), (pltpu.VMEM((5, 2 * NC, C), F32),), 4e9, limit=54, split=OUTER_SPLIT,
    )
    *a_in, decay_grad = lax.optimization_barrier((*a_in, decay_grad))
    a_sum = a[0] + a_in[0] + a_in[1] + a_in[2]
    b_sum = b[0] + b_in[0] + b_in[1] + b_in[2]
    piece = lambda acc, i: lax.dynamic_index_in_dim(acc, i, 0, keepdims=False)
    a_last = [piece(a_sum, x)] + [lax.ppermute(piece(a_sum, (x + d) % 4), "sp", ring(d, False)) for d in (1, 3, 2)]
    b_last = [piece(b_sum, z)] + [lax.ppermute(piece(b_sum, (z + d) % 4), "sp", ring(d, True)) for d in (1, 3, 2)]

    weight_grad, norms = pl.pallas_call(
        finish_kernel, out_shape=(sds((256, WIDE)), sds((2, HALF))), in_specs=[VMEM] * 8, out_specs=(VMEM, VMEM),
        name="finish", compiler_params=pltpu.CompilerParams(vmem_limit_bytes=4 * 1024 * 1024),
    )(*a_last, *b_last)
    norms = norms + lax.ppermute(norms, "tp", [(i, i ^ 1) for i in range(8)])
    others = [lax.ppermute(norms, "tp", [(i, (i + 2 * d) % 8) for i in range(8)]) for d in (2, 1, 3)]
    norms = norms + others[0] + others[1] + others[2]
    return key_grad.T, query_grad.T, decay_grad, gate_grad, weight_grad, norms.reshape(256)


def solution(mesh):
    in_specs = (
        P("sp", None), P(None, "tp"), P("sp", "tp"), P("sp", "tp"), P("tp", "sp"), P("tp"), P("sp", "tp"), P("sp", "tp"),
    )
    out_specs = (P("sp", "tp"), P("sp", "tp"), P("tp", "sp"), P("sp", "tp"), P("sp", "tp"), P("sp"))
    return jax.shard_map(shards, mesh=mesh, in_specs=in_specs, out_specs=out_specs, check_vma=False)
```
